128 devices in a mesh: ep: 128 (over z, y, x, core).
Axes of the slice: x: 4, y: 4, z: 4, core: 2. Of those that a mesh axis runs over, the one named last changes fastest.
Arguments:
- hidden_in: bfloat16 [256, 2048], P('ep'), may hold values from -6 to 6
- lengths: int32 [256], P('ep'), may hold values from 1 to 1024, as said below
- key_cache: bfloat16 [256, 1024, 512], P('ep'), may hold values from -30 to 30
- value_cache: bfloat16 [256, 1024, 512], P('ep'), may hold values from -6 to 6
- query_w: bfloat16 [2048, 2048], P('ep'), may hold values from -0.125 to 0.125
- key_w: bfloat16 [2048, 512], P('ep'), may hold values from -0.125 to 0.125
- value_w: bfloat16 [2048, 512], P('ep'), may hold values from -0.125 to 0.125
- out_w: bfloat16 [2048, 2048], P('ep'), may hold values from -0.125 to 0.125
- lam_heads: float32 [8], replicated, may hold values from 0.3 to 0.8
- head_gain: float32 [256], replicated, may hold values from 0.1 to 1.9
- attn_gain: float32 [2048], replicated, may hold values from 0.1 to 1.9
- moe_gain: float32 [2048], replicated, may hold values from 0.1 to 1.9
- routing: int32 [256, 6], replicated, may hold values from 0 to 127, all different within a row; in each aligned block of 256 rows (0 to 255, 256 to 511, ...) at most 24 rows name the same one
- route_weight: float32 [256, 6], replicated, may hold values from 0.1 to 0.6
- gate_w: bfloat16 [128, 2048, 512], P('ep'), may hold values from -0.125 to 0.125
- up_w: bfloat16 [128, 2048, 512], P('ep'), may hold values from -0.125 to 0.125
- down_w: bfloat16 [128, 512, 2048], P('ep'), may hold values from -0.25 to 0.25
- shared_gate: bfloat16 [2048, 512], replicated, may hold values from -0.125 to 0.125
- shared_up: bfloat16 [2048, 512], replicated, may hold values from -0.125 to 0.125
- shared_down: bfloat16 [512, 2048], replicated, may hold values from -0.25 to 0.25
Outputs:
- layer_out: bfloat16 [256, 2048], P('ep')
- key_new: bfloat16 [256, 512], P('ep')
- value_new: bfloat16 [256, 512], P('ep')
The draws below stay inside these ranges and needn't reach their ends.
Inputs may be any that keep to these rules, and one draw needn't show every extreme that they name: `lengths`: some sequence has exactly 1024 positions in use. `routing`: each row names 6 different experts; no expert is named by more than 24 rows, a bound that some block reaches.
All inputs are finite; a program needn't handle non-finite values.
Results may differ from the reference program's by a relative error of at most 0.013.
The reference program's roundings to bfloat16 on the way count: a program that leaves them out, or rounds other values in their place, can miss the bound.
Values may be sent and summed in bfloat16 or wider, within the bound.
A program may use at most 64 MiB of HBM per device.

```python
import math
import jax
import jax.numpy as jnp
import numpy as np
from jax import lax

D = 2048
HEADS = 8
KV_HEADS = 2
HEAD_DIM = 128
VALUE_DIM = 256
EXPERT_DIM = 512
SHARED_DIM = 512
TOPK = 6
CACHE = 1024
SEQS = 256
EXPERTS = 128
EXP_CAP = 24


def draw_lengths(key, part):
    first_key, second_key = jax.random.split(key, 2)
    drawn = jax.random.randint(first_key, (SEQS,), 1, CACHE + 1, jnp.int32)
    chosen = jax.random.randint(second_key, (), 0, SEQS, jnp.int32)
    return jnp.where(jnp.arange(SEQS, dtype=jnp.int32) == chosen, CACHE, drawn).astype(jnp.int32)


def draw_key_cache(key, part):
    first_key = jax.random.fold_in(key, 0)
    shape = (SEQS, CACHE, KV_HEADS * 2 * HEAD_DIM)
    drawn = jnp.clip(1.75 * jax.random.normal(first_key, shape, jnp.float32), -14.0, 14.0)
    return drawn.astype(jnp.bfloat16)


def block_levels(own_key, extent, cuts, smallest, high):
    factor_of = 1.0
    for axis_at, shards_of in cuts:
        heights = jax.random.uniform(jax.random.fold_in(jax.random.fold_in(own_key, 6), axis_at), (shards_of,), jnp.float32, smallest / len(cuts), high / len(cuts))
        factor_of = factor_of * jnp.repeat(jnp.exp(heights), extent[axis_at] // shards_of).reshape((-1,) + (1,) * (len(extent) - 1 - axis_at))
    return factor_of


def deal_out(stream_key, own, number, rows, count, top, reach, slope):
    ranking = jax.random.permutation(stream_key, count)
    packed, ordinary = shares(count, rows * top, reach, slope, True), shares(count, rows * top, reach, slope, False)
    places = jnp.arange(count)

    def named(tallies, offset_by):
        used = int((tallies > 0).sum())
        fixed = max(1, used // 4)
        shifted = fixed + (places - fixed + offset_by * (used - fixed)) % max(1, count - fixed)
        return jnp.zeros((count,), jnp.int32).at[ranking[jnp.where(places < fixed, places, shifted)]].set(jnp.asarray(tallies, jnp.int32))

    tallies = jnp.where(number % 4 == 0, named(packed, number // 4), named(ordinary, number - number // 4 - 1))
    mixed = jax.random.permutation(jax.random.fold_in(own, 3), count)
    donor, receiver = mixed[0:count // 2 * 2:2], mixed[1:count // 2 * 2:2]
    margin = jnp.minimum(tallies[donor] - 1, reach - tallies[receiver]) // 2
    margin = jnp.where((donor == ranking[0]) | (receiver == ranking[0]) | (tallies[receiver] == 0), 0, jnp.maximum(margin, 0))
    shifted = jax.random.randint(jax.random.fold_in(own, 4), (count // 2,), 0, 1 << 20) % (margin + 1)
    tallies = tallies.at[donor].add(-shifted).at[receiver].add(shifted)
    items = jnp.searchsorted(jnp.cumsum(tallies), jnp.arange(rows * top), side="right").astype(jnp.int32)
    table = items.reshape(top, rows).T
    table = table[jax.random.permutation(jax.random.fold_in(own, 1), rows)]
    offset_by = jax.random.randint(jax.random.fold_in(own, 2), (rows, 1), 0, top)
    return jnp.take_along_axis(table, (jnp.arange(top)[None, :] + offset_by) % top, axis=1)


def shares(number_of, total, bound, lean, full):
    portions = [(1 << 20) // math.isqrt(grade ** lean) + 1 for grade in range(1, number_of + 1)]
    largest = bound if full else min(bound, max(-(-total // number_of), total * portions[0] // sum(portions)))
    least = 1 if total - largest >= number_of - 1 else 0
    counts, surplus = [largest] + [least] * (number_of - 1), total - largest - least * (number_of - 1)
    while surplus > 0:
        candidates = [i for i in range(1, number_of) if counts[i] < largest] or [i for i in range(1, number_of) if counts[i] < bound]
        whole, left = sum([portions[i] for i in candidates]), surplus
        for i in candidates:
            more = min(bound - counts[i], max(1, left * portions[i] // whole), surplus)
            counts[i] = counts[i] + more
            surplus = surplus - more
    return np.array(counts)


def noise(stream_key, shape, scale, most, pieces=(), kind=jnp.bfloat16):
    values = jax.random.normal(stream_key, shape, jnp.float32) * scale
    if len(pieces) > 0:
        values = block_levels(stream_key, shape, pieces, -0.22, 0.18) * values
    return jnp.clip(values, min=-most, max=most).astype(kind)


def setup_inputs(seed: int = 0) -> dict:
    key_list = jax.random.split(jax.random.key(seed), 21)
    hidden_in = noise(key_list[0], (SEQS, D), 1.0, 6.0, ((0, 128),))
    lengths = draw_lengths(jax.random.fold_in(key_list[20], 71), 0)
    key_cache = draw_key_cache(jax.random.fold_in(key_list[20], 71), 0)
    value_cache = noise(key_list[3], (SEQS, CACHE, KV_HEADS * VALUE_DIM), 1.0, 6.0, ((0, 128),))
    query_w = noise(key_list[4], (D, HEADS * 2 * HEAD_DIM), D ** -0.5, 0.125, ((0, 128),))
    key_w = noise(key_list[5], (D, KV_HEADS * 2 * HEAD_DIM), D ** -0.5, 0.125, ((0, 128),))
    value_w = noise(key_list[6], (D, KV_HEADS * VALUE_DIM), D ** -0.5, 0.125, ((0, 128),))
    out_w = noise(key_list[7], (HEADS * VALUE_DIM, D), (HEADS * VALUE_DIM) ** -0.5, 0.125, ((0, 128),))
    lam_heads = jnp.clip(jax.random.uniform(key_list[8], (HEADS,), jnp.float32, 0.3, 0.8), 0.3, 0.8)
    head_gain = jnp.clip(1.0 + 0.18 * jax.random.normal(key_list[9], (VALUE_DIM,), jnp.float32), 0.1, 1.9)
    attn_gain = jnp.clip(1.0 + 0.18 * jax.random.normal(key_list[10], (D,), jnp.float32), 0.1, 1.9)
    moe_gain = jnp.clip(1.0 + 0.18 * jax.random.normal(key_list[11], (D,), jnp.float32), 0.1, 1.9)
    routing_keys = jax.random.split(jax.random.fold_in(key_list[12], 1), SEQS // SEQS)
    routing_turns = jax.random.permutation(jax.random.fold_in(key_list[12], 3), SEQS // SEQS)
    routing = jax.vmap(lambda own, number: deal_out(jax.random.fold_in(key_list[12], 2), own, number, SEQS, EXPERTS, TOPK, EXP_CAP, 1))(routing_keys, routing_turns).reshape((SEQS, TOPK))
    route_weight = jnp.clip(jnp.exp(jax.random.uniform(key_list[13], (SEQS, TOPK), jnp.float32, math.log(0.1), math.log(0.6))), 0.1, 0.6)
    gate_w = noise(key_list[14], (EXPERTS, D, EXPERT_DIM), D ** -0.5, 0.125, ((0, 128),))
    up_w = noise(key_list[15], (EXPERTS, D, EXPERT_DIM), D ** -0.5, 0.125, ((0, 128),))
    down_w = noise(key_list[16], (EXPERTS, EXPERT_DIM, D), EXPERT_DIM ** -0.5, 0.25, ((0, 128),))
    shared_gate = noise(key_list[17], (D, SHARED_DIM), D ** -0.5, 0.125)
    shared_up = noise(key_list[18], (D, SHARED_DIM), D ** -0.5, 0.125)
    shared_down = noise(key_list[19], (SHARED_DIM, D), SHARED_DIM ** -0.5, 0.25)
    return dict(hidden_in=hidden_in, lengths=lengths, key_cache=key_cache, value_cache=value_cache, query_w=query_w, key_w=key_w, value_w=value_w, out_w=out_w, lam_heads=lam_heads, head_gain=head_gain, attn_gain=attn_gain, moe_gain=moe_gain, routing=routing, route_weight=route_weight, gate_w=gate_w, up_w=up_w, down_w=down_w, shared_gate=shared_gate, shared_up=shared_up, shared_down=shared_down)


eps_norm = 1e-06
eps_head = 1e-05
theta_base = 500000.0

def rms_scale(row_block, gain_vec, epsilon):
    row_block = row_block.astype(jnp.float32)
    return row_block * lax.rsqrt(lax.optimization_barrier(jnp.mean(row_block * row_block, axis=-1, keepdims=True)) + epsilon) * gain_vec.astype(jnp.float32)

def rotate(vectors, positions):
    half_width = vectors.shape[-1] // 2
    inverse = theta_base ** (-jnp.arange(half_width, dtype=jnp.float32) / half_width)
    angles = positions.astype(jnp.float32)[..., None] * inverse
    cosine, sine_part = (jnp.cos(angles), jnp.sin(angles))
    lower_half, upper_half = (vectors[..., :half_width], vectors[..., half_width:])
    return jnp.concatenate([lower_half * cosine - upper_half * sine_part, lower_half * sine_part + upper_half * cosine], axis=-1)

def attend(queries, key_new, value_new, cache_keys, cache_values, lengths, lam_heads, head_gain):
    num_seqs, kv_heads, group_size = (queries.shape[0], queries.shape[1], queries.shape[2])
    head_dim = queries.shape[-1]
    cache_len = cache_keys.shape[1]
    cache_keys = cache_keys.reshape(num_seqs, cache_len, kv_heads, 2, head_dim).astype(jnp.float32)
    cache_values = cache_values.reshape(num_seqs, cache_len, kv_heads, -1).astype(jnp.float32)
    value_new = value_new.reshape(num_seqs, kv_heads, -1)
    queries = queries.astype(jnp.float32)
    score_scale = head_dim ** (-0.5)
    scores = jnp.einsum('skgph,sckph->skgpc', queries, cache_keys) * score_scale
    self_score = jnp.einsum('skgph,skph->skgp', queries, key_new.astype(jnp.float32)) * score_scale
    live_mask = (jnp.arange(cache_len)[None, :] < lengths[:, None])[:, None, None, None, :]
    peak = jnp.maximum(lax.optimization_barrier(jnp.max(jnp.where(live_mask, scores, -jnp.inf), axis=-1)), self_score)
    weights = jnp.where(live_mask, jnp.exp(scores - peak[..., None]), 0.0)
    self_weight = jnp.exp(self_score - peak)
    totals = lax.optimization_barrier(jnp.sum(weights, axis=-1)) + self_weight
    lambda_grid = lam_heads.reshape(kv_heads, group_size)[None]
    combined = (weights[:, :, :, 0] / totals[:, :, :, 0, None] - lambda_grid[..., None] * weights[:, :, :, 1] / totals[:, :, :, 1, None]).astype(jnp.bfloat16)
    self_combined = (self_weight[..., 0] / totals[..., 0] - lambda_grid * self_weight[..., 1] / totals[..., 1]).astype(jnp.bfloat16)
    head_out = jnp.einsum('skgc,sckv->skgv', combined.astype(jnp.float32), cache_values)
    head_out = head_out + self_combined.astype(jnp.float32)[..., None] * value_new.astype(jnp.float32)[:, :, None, :]
    return rms_scale(head_out, head_gain, eps_head).astype(jnp.bfloat16).reshape(num_seqs, -1)

def routed_sum(moe_in, routing, route_weight, gate_w, up_w, down_w):

    def add_expert(running, expert_id):
        routed_here = lax.optimization_barrier(jnp.sum((routing == expert_id).astype(jnp.int32), axis=1))
        weight_col = lax.optimization_barrier(jnp.sum(jnp.where(routing == expert_id, route_weight, 0.0), axis=1))
        slot_index = jnp.cumsum(routed_here) - 1
        pick_table = ((slot_index[None, :] == jnp.arange(EXP_CAP)[:, None]) & (routed_here[None, :] > 0)).astype(jnp.float32)
        picked = jnp.dot(pick_table, moe_in.astype(jnp.float32)).astype(jnp.bfloat16)
        gate_one = lax.dynamic_index_in_dim(gate_w, expert_id, 0, keepdims=False)
        up_one = lax.dynamic_index_in_dim(up_w, expert_id, 0, keepdims=False)
        down_one = lax.dynamic_index_in_dim(down_w, expert_id, 0, keepdims=False)
        hidden = (jax.nn.silu(jnp.dot(picked, gate_one, preferred_element_type=jnp.float32)) * jnp.dot(picked, up_one, preferred_element_type=jnp.float32)).astype(jnp.bfloat16)
        result = jnp.dot(hidden, down_one, preferred_element_type=jnp.float32).astype(jnp.bfloat16)
        return (running + jnp.dot(pick_table.T, result.astype(jnp.float32)) * weight_col[:, None], None)
    start_sum = jnp.zeros(moe_in.shape, jnp.float32)
    running, unused = lax.scan(add_expert, start_sum, jnp.arange(gate_w.shape[0], dtype=jnp.int32))
    return running

def reference(hidden_in, lengths, key_cache, value_cache, query_w, key_w, value_w, out_w, lam_heads, head_gain, attn_gain, moe_gain, routing, route_weight, gate_w, up_w, down_w, shared_gate, shared_up, shared_down):
    num_seqs = hidden_in.shape[0]
    normed = rms_scale(hidden_in, attn_gain, eps_norm).astype(jnp.bfloat16)
    q_raw = jnp.dot(normed, query_w, preferred_element_type=jnp.float32)
    k_raw = jnp.dot(normed, key_w, preferred_element_type=jnp.float32)
    value_new = jnp.dot(normed, value_w, preferred_element_type=jnp.float32).astype(jnp.bfloat16)
    queries = rotate(q_raw.reshape(num_seqs, KV_HEADS, -1, 2, HEAD_DIM), lengths[:, None, None, None]).astype(jnp.bfloat16)
    key_new = rotate(k_raw.reshape(num_seqs, KV_HEADS, 2, HEAD_DIM), lengths[:, None, None]).astype(jnp.bfloat16)

    def one_sequence(items):
        return attend(*[item[None] for item in items], lam_heads, head_gain)[0]
    attn_out = lax.map(one_sequence, (queries, key_new, value_new, key_cache, value_cache, lengths))
    attn_proj = jnp.dot(attn_out, out_w, preferred_element_type=jnp.float32).astype(jnp.bfloat16)
    after_mixer = (hidden_in.astype(jnp.float32) + attn_proj.astype(jnp.float32)).astype(jnp.bfloat16)
    moe_in = rms_scale(after_mixer, moe_gain, eps_norm).astype(jnp.bfloat16)
    routed = routed_sum(moe_in, routing, route_weight, gate_w, up_w, down_w)
    shared_hidden = (jax.nn.silu(jnp.dot(moe_in, shared_gate, preferred_element_type=jnp.float32)) * jnp.dot(moe_in, shared_up, preferred_element_type=jnp.float32)).astype(jnp.bfloat16)
    shared_out = jnp.dot(shared_hidden, shared_down, preferred_element_type=jnp.float32)
    layer_out = (after_mixer.astype(jnp.float32) + routed + shared_out).astype(jnp.bfloat16)
    return (layer_out, key_new.reshape(num_seqs, -1), value_new)
```

```python
import functools

import jax
import jax.numpy as jnp
import numpy as np
from jax import lax
from jax.experimental import pallas as pl
from jax.experimental.pallas import tpu as pltpu
from jax.sharding import PartitionSpec as P

MESH = pl.DeviceIdType.MESH
F32 = jnp.float32
BF16 = jnp.bfloat16
SIDE = 4
CHIPS = SIDE**3
PLANE = SIDE * SIDE * 2
SLOTS = 32
D = 2048
eps_norm = 1e-06
eps_head = 1e-05
theta_base = 500000.0


def bytes_of(buf, count, sem):
    part = buf.at[pl.ds(0, count)]
    pltpu.make_async_copy(part, part, sem).wait()


def row_parity():
    return lax.broadcasted_iota(jnp.int32, (32, 128), 0) % 2


def fold_rms(fold, gain):
    parity = row_parity()
    squares = fold * fold
    first = jnp.sum(jnp.where(parity == 0, squares, 0.0), keepdims=True)
    second = jnp.sum(jnp.where(parity == 1, squares, 0.0), keepdims=True)
    r0 = lax.rsqrt(first * (1.0 / D) + eps_norm)
    r1 = lax.rsqrt(second * (1.0 / D) + eps_norm)
    return fold * jnp.where(parity == 0, r0, r1) * gain


def kernel(
    len_ref, lam_ref, hidden_ref, inv_ref, again_ref, mgain_ref, hgain_ref, routing_ref, rweight_ref,
    kc_hbm, vc_hbm, qw_hbm, kw_hbm, vw_hbm, ow_hbm, gate_hbm, up_hbm, down_hbm, sg_hbm, su_hbm, sd_hbm,
    layer_ref, kout_ref, vout_ref,
    kc, vc, gate, up, down, sg, su, sd,
    wcat, owcat, wrecv, owrecv,
    hid, gdup, asend, acts, xf, p2, qkv_in, qs,
    af, asend2, acts2, p5, oin, proj,
    ms, mrecv, big, pk, rs, rpar, esend, erecv, es, shf, rfold,
    pt, ptt, wtok, ptmp,
    local_sem, send_sem, recv_sem,
):
    me = lax.axis_index("ep")
    c = me % 2
    p = me // 2
    x = p % SIDE
    y = (p // SIDE) % SIDE
    z = p // (SIDE * SIDE)
    xc = x * 2 + c
    partner = me + 1 - 2 * c
    o_me = z * 8 + xc
    w_me = y * 8 + xc

    def local(src, dst, k):
        cp = pltpu.make_async_copy(src, dst, local_sem.at[k])
        cp.start()
        return cp

    def remote(src, dst, k, target):
        pltpu.make_async_remote_copy(
            src_ref=src,
            dst_ref=dst,
            send_sem=send_sem.at[k],
            recv_sem=recv_sem.at[k],
            device_id=(target,),
            device_id_type=MESH,
        ).start()

    for h in range(8):
        local(qw_hbm.at[:, pl.ds(h * 256, 256)], wcat.at[h, :, pl.ds(0, 256)], 0)
        kv_hbm = kw_hbm if h < 4 else vw_hbm
        local(kv_hbm.at[:, pl.ds((h % 4) * 128, 128)], wcat.at[h, :, pl.ds(256, 128)], 0)
    for h in range(8):
        local(ow_hbm.at[:, pl.ds(h * 256, 256)], owcat.at[h], 1)
    c_kc = local(kc_hbm, kc, 2)
    c_vc = local(vc_hbm, vc, 3)
    c_sg = local(sg_hbm, sg, 4)
    c_su = local(su_hbm, su, 5)
    c_sd = local(sd_hbm, sd, 6)
    c_gate = local(gate_hbm.at[0], gate, 7)
    c_up = local(up_hbm.at[0], up, 8)
    c_down = local(down_hbm.at[0], down, 9)

    barrier = pltpu.get_barrier_semaphore()

    def greet(k, _):
        pl.semaphore_signal(
            barrier, inc=1, device_id=((me + k) % (2 * CHIPS),), device_id_type=MESH
        )
        return 0

    lax.fori_loop(1, 2 * CHIPS, greet, 0)

    wide = hidden_ref[...].astype(F32)
    for s in range(16):
        hid[2 * s : 2 * s + 2, :] = wide[:, 128 * s : 128 * s + 128]
    hidden = hid[...]

    def doubled(gain_ref):
        gdup[pl.ds(0, 16, stride=2), :] = gain_ref[...]
        gdup[pl.ds(1, 16, stride=2), :] = gain_ref[...]
        return gdup[...]

    asend[...] = fold_rms(hidden, doubled(again_ref)).astype(BF16).reshape(4, 8, 128)
    pltpu.make_async_copy(wcat, wcat, local_sem.at[0]).wait()
    pl.semaphore_wait(barrier, 2 * CHIPS - 1)

    def owner_of(k):
        dz, dx, dc = k // 8, (k // 2) % 4, k % 2
        zt, xt, ct = (z + dz) % SIDE, (x + dx) % SIDE, (c + dc) % 2
        return zt, xt * 2 + ct, ((zt * SIDE + y) * SIDE + xt) * 2 + ct

    def holder_of(k):
        dy, dx, dc = k // 8, (k // 2) % 4, k % 2
        yt, xt, ct = (y + dy) % SIDE, (x + dx) % SIDE, (c + dc) % 2
        return xt * 2 + ct, ((z * SIDE + yt) * SIDE + xt) * 2 + ct

    def chip_of(k):
        dz, dy, dx = k // 16, (k // 4) % 4, k % 4
        return (((z + dz) % SIDE) * SIDE + (y + dy) % SIDE) * SIDE + (x + dx) % SIDE

    def send_acts(k, _):
        zt, _, target = owner_of(k)
        remote(asend.at[zt], acts.at[o_me], 0, target)
        return 0

    def send_w(k, _):
        ht, target = holder_of(k)
        remote(wcat.at[ht], wrecv.at[w_me], 1, target)
        return 0

    lax.fori_loop(1, PLANE, send_acts, 0)
    lax.fori_loop(1, PLANE, send_w, 0)
    acts[o_me] = asend[z]
    wrecv[w_me] = wcat[xc]

    lane = lax.broadcasted_iota(jnp.int32, (256, 128), 1)
    tri = (
        lax.broadcasted_iota(jnp.int32, (256, 256), 1)
        <= lax.broadcasted_iota(jnp.int32, (256, 256), 0)
    ).astype(BF16)
    for i in range(2):
        expert = me if i == 0 else partner
        match = routing_ref[...] == expert
        here = jnp.max(jnp.where(match, 1.0, 0.0), axis=1, keepdims=True)
        weight = jnp.sum(jnp.where(match, rweight_ref[...], 0.0), axis=1, keepdims=True)
        spread = jnp.broadcast_to(here, (256, 128))
        place = jnp.dot(tri, spread.astype(BF16), preferred_element_type=F32) - 1.0
        table = jnp.where((place == lane.astype(F32)) & (spread > 0.0), 1.0, 0.0)
        ptmp[...] = table
        for ct in range(4):
            pt[i, ct * 64 : ct * 64 + 64, :] = ptmp[pl.ds(ct, 64, stride=4), :]
        ptmp[...] = jnp.broadcast_to(weight, (256, 128))
        for ct in range(4):
            wtok[i, ct * 64 : ct * 64 + 64, :] = ptmp[pl.ds(ct, 64, stride=4), :]
    ptt[...] = jnp.transpose(pt[0])[0:SLOTS].astype(BF16)

    half_sign = jnp.where(lax.broadcasted_iota(jnp.int32, (1, 128), 1) < 64, -1.0, 1.0)
    turns = []
    for t in range(2):
        angle = len_ref[t].astype(F32) * inv_ref[...]
        turns.append((jnp.cos(angle), jnp.sin(angle) * half_sign))

    def columns_of(arrived):
        xf[...] = arrived[...].astype(F32).reshape(256, 128)
        rows = [
            jnp.concatenate(
                [xf[pl.ds(2 * s + t, 32, stride=8), :] for t in range(2)], axis=0
            )
            for s in range(4)
        ]
        return jnp.concatenate(rows, axis=1).astype(BF16)

    bytes_of(acts, PLANE - 1, recv_sem.at[0])
    bytes_of(wrecv, PLANE - 1, recv_sem.at[1])
    part = jnp.dot(
        columns_of(acts), wrecv[...].reshape(512, 384), preferred_element_type=F32
    )
    for b in range(3):
        for t in range(2):
            p2[pl.ds(2 * b + t, 32, stride=8), :] = part[
                32 * t : 32 * t + 32, 128 * b : 128 * b + 128
            ]
    for t in range(2):
        p2[pl.ds(6 + t, 32, stride=8), :] = jnp.zeros((32, 128), F32)

    def send_part(k, _):
        zt, ht, target = owner_of(k)
        ot = pl.multiple_of((zt * 8 + ht) * 8, 8)
        remote(p2.at[pl.ds(ot, 8), :], qkv_in.at[o_me], 2, target)
        return 0

    lax.fori_loop(1, PLANE, send_part, 0)
    qkv_in[o_me] = p2[pl.ds(pl.multiple_of(o_me * 8, 8), 8), :]

    pltpu.make_async_copy(owcat, owcat, local_sem.at[1]).wait()

    def send_ow(k, _):
        ht, target = holder_of(k)
        remote(owcat.at[ht], owrecv.at[w_me], 3, target)
        return 0

    lax.fori_loop(1, PLANE, send_ow, 0)
    owrecv[w_me] = owcat[xc]
    c_kc.wait()
    c_vc.wait()

    bytes_of(qkv_in, PLANE - 1, recv_sem.at[2])
    total = qkv_in[0:8]
    for k in range(1, 4):
        total = total + qkv_in[8 * k : 8 * k + 8]
    qs[...] = total.reshape(64, 128)

    scale = 128.0**-0.5
    row16 = lax.broadcasted_iota(jnp.int32, (16, 128), 0)
    row8 = lax.broadcasted_iota(jnp.int32, (8, 1), 0)
    lam = jnp.zeros((8, 1), F32)
    for h in range(8):
        lam = jnp.where(row8 == h, lam_ref[h], lam)
    keys, values = [], []
    for t in range(2):
        cos, sin = turns[t]

        def turn(v):
            return v * cos + pltpu.roll(v, 64, 1) * sin

        kv = qs[pl.ds(4 + t, 8, stride=8), :]
        q16 = jnp.concatenate(
            [turn(qs[pl.ds(t, 8, stride=8), :]), turn(qs[pl.ds(2 + t, 8, stride=8), :])],
            axis=0,
        )
        q16 = q16.astype(BF16).astype(F32)
        kn = turn(kv).astype(BF16).astype(F32)
        vn = kv.astype(BF16).astype(F32)
        keys.append(jnp.concatenate([kn[i : i + 1] for i in range(4)], axis=1))
        vflat = jnp.concatenate([vn[i : i + 1] for i in range(4, 8)], axis=1)
        values.append(vflat)
        own_keys = jnp.concatenate(
            [jnp.broadcast_to(kn[i : i + 1], (4, 128)) for i in (0, 2, 1, 3)], axis=0
        )
        self_score = jnp.sum(q16 * own_keys, axis=1, keepdims=True) * scale
        blocks = []
        for k in range(2):
            for j in range(2):
                lo = j * 8 + k * 4
                blocks.append(jnp.where((row16 >= lo) & (row16 < lo + 4), q16, 0.0))
        wide_q = jnp.concatenate(blocks, axis=1).astype(BF16)
        scores = (
            lax.dot_general(
                wide_q, kc[t], (((1,), (1,)), ((), ())), preferred_element_type=F32
            )
            * scale
        )
        live = lax.broadcasted_iota(jnp.int32, (16, 1024), 1) < len_ref[t]
        peak = jnp.maximum(
            jnp.max(jnp.where(live, scores, -jnp.inf), axis=1, keepdims=True), self_score
        )
        weights = jnp.where(live, jnp.exp(scores - peak), 0.0)
        self_w = jnp.exp(self_score - peak)
        totals = jnp.sum(weights, axis=1, keepdims=True) + self_w
        comb = weights[0:8] / totals[0:8] - lam * weights[8:16] / totals[8:16]
        self_comb = self_w[0:8] / totals[0:8] - lam * self_w[8:16] / totals[8:16]
        out = jnp.dot(comb.astype(BF16), vc[t], preferred_element_type=F32)
        out = out + self_comb.astype(BF16).astype(F32) * vflat
        head = jnp.where(row8 < 4, out[:, 0:256], out[:, 256:512])
        mean = jnp.sum(head * head, axis=1, keepdims=True) * (1.0 / 256)
        head = head * lax.rsqrt(mean + eps_head) * hgain_ref[...]
        for half in range(2):
            af[pl.ds(2 * half + t, 8, stride=4), :] = head[:, 128 * half : 128 * half + 128]
    kout_ref[...] = jnp.concatenate(keys, axis=0).astype(BF16)
    vout_ref[...] = jnp.concatenate(values, axis=0).astype(BF16)
    asend2[...] = af[...].astype(BF16).reshape(4, 8, 128)

    def send_acts2(k, _):
        zt, _, target = owner_of(k)
        remote(asend2.at[zt], acts2.at[o_me], 4, target)
        return 0

    lax.fori_loop(1, PLANE, send_acts2, 0)
    acts2[o_me] = asend2[z]
    mgain = doubled(mgain_ref)
    bytes_of(owrecv, PLANE - 1, recv_sem.at[3])
    bytes_of(acts2, PLANE - 1, recv_sem.at[4])
    part = jnp.dot(
        columns_of(acts2), owrecv[...].reshape(512, 256), preferred_element_type=F32
    )
    for b in range(2):
        for t in range(2):
            p5[pl.ds(2 * b + t, 32, stride=8), :] = part[
                32 * t : 32 * t + 32, 128 * b : 128 * b + 128
            ]
    for r in range(4, 8):
        p5[pl.ds(r, 32, stride=8), :] = jnp.zeros((32, 128), F32)

    def send_part2(k, _):
        zt, ht, target = owner_of(k)
        ot = pl.multiple_of((zt * 8 + ht) * 8, 8)
        remote(p5.at[pl.ds(ot, 8), :], oin.at[o_me], 5, target)
        return 0

    lax.fori_loop(1, PLANE, send_part2, 0)
    oin[o_me] = p5[pl.ds(pl.multiple_of(o_me * 8, 8), 8), :]
    bytes_of(oin, PLANE - 1, recv_sem.at[5])
    total = oin[0:8]
    for k in range(1, 4):
        total = total + oin[8 * k : 8 * k + 8]
    for h in range(8):
        proj[4 * h : 4 * h + 4, :] = total[h, 0:4]
    mixed = (hidden + proj[...].astype(BF16).astype(F32)).astype(BF16).astype(F32)
    moe = fold_rms(mixed, mgain).astype(BF16)
    ms[...] = moe

    def send_moe(k, _):
        remote(ms, mrecv.at[c, p], 6, chip_of(k) * 2 + c)
        return 0

    lax.fori_loop(1, CHIPS, send_moe, 0)
    mrecv[c, p] = moe

    moe32 = moe.astype(F32)
    lhs = jnp.concatenate([moe32[2 * s : 2 * s + 2] for s in range(16)], axis=1).astype(BF16)
    c_sg.wait()
    c_su.wait()
    c_sd.wait()
    g = jnp.dot(lhs, sg[...], preferred_element_type=F32)
    u = jnp.dot(lhs, su[...], preferred_element_type=F32)
    shared = jnp.dot(
        (jax.nn.silu(g) * u).astype(BF16), sd[...], preferred_element_type=F32
    )
    for s in range(16):
        shf[2 * s : 2 * s + 2, :] = shared[:, 128 * s : 128 * s + 128]
    c_gate.wait()
    c_up.wait()
    c_down.wait()

    bytes_of(mrecv.at[0], CHIPS - 1, recv_sem.at[6])
    remote(mrecv.at[c], mrecv.at[c], 7, partner)

    def widen_own(i, _):
        big[pl.ds(pl.multiple_of(c * 2048 + i * 128, 128), 128), :] = (
            mrecv[c, pl.ds(i * 4, 4)].astype(F32).reshape(128, 128)
        )
        return 0

    lax.fori_loop(0, 16, widen_own, 0)
    bytes_of(mrecv.at[0], CHIPS, recv_sem.at[7])

    def widen_other(i, _):
        big[pl.ds(pl.multiple_of((1 - c) * 2048 + i * 128, 128), 128), :] = (
            mrecv[1 - c, pl.ds(i * 4, 4)].astype(F32).reshape(128, 128)
        )
        return 0

    lax.fori_loop(0, 16, widen_other, 0)
    for s in range(16):
        rows = jnp.concatenate(
            [
                big[pl.ds((ct // 2) * 2048 + 2 * s + ct % 2, 64, stride=32), :]
                for ct in range(4)
            ],
            axis=0,
        ).astype(BF16)
        pk[:, 128 * s : 128 * s + 128] = jnp.dot(
            ptt[...], rows, preferred_element_type=F32
        ).astype(BF16)
    g = jnp.dot(pk[...], gate[...], preferred_element_type=F32)
    u = jnp.dot(pk[...], up[...], preferred_element_type=F32)
    hidden_e = (jax.nn.silu(g) * u).astype(BF16)
    for i in range(2):
        rs[i] = jnp.dot(
            hidden_e, down[:, 1024 * i : 1024 * i + 1024], preferred_element_type=F32
        ).astype(BF16)

    remote(rs.at[1 - c], rpar, 8, partner)
    own = jnp.dot(pt[0, :, 0:SLOTS].astype(BF16), rs[c], preferred_element_type=F32)
    for ct in range(4):
        for s in range(8):
            big[pl.ds(4 * s + ct, 64, stride=32), :] = (
                own[64 * ct : 64 * ct + 64, 128 * s : 128 * s + 128]
                * wtok[0, 64 * ct : 64 * ct + 64, :]
            )
    bytes_of(rpar, SLOTS, recv_sem.at[8])
    other = jnp.dot(pt[1, :, 0:SLOTS].astype(BF16), rpar[...], preferred_element_type=F32)
    for ct in range(4):
        for s in range(8):
            big[pl.ds(4 * s + ct, 64, stride=32), :] = (
                big[pl.ds(4 * s + ct, 64, stride=32), :]
                + other[64 * ct : 64 * ct + 64, 128 * s : 128 * s + 128]
                * wtok[1, 64 * ct : 64 * ct + 64, :]
            )

    def narrow(i, _):
        esend[pl.ds(i * 4, 4)] = (
            big[pl.ds(pl.multiple_of(i * 128, 128), 128), :].astype(BF16).reshape(4, 32, 128)
        )
        return 0

    lax.fori_loop(0, 16, narrow, 0)

    def send_back(k, _):
        chip = chip_of(k)
        remote(esend.at[chip], erecv.at[p], 9, chip * 2 + c)
        return 0

    lax.fori_loop(1, CHIPS, send_back, 0)
    erecv[p] = esend[p]
    bytes_of(erecv, CHIPS - 1, recv_sem.at[9])

    def add_up(i, acc):
        return acc + jnp.sum(erecv[pl.ds(i * 4, 4)].astype(F32), axis=0)

    total = lax.fori_loop(0, 16, add_up, jnp.zeros((32, 128), F32))
    mine = pl.multiple_of(c * 32, 32)
    es[pl.ds(mine, 32), :] = total
    remote(es.at[pl.ds(mine, 32), :], es.at[pl.ds(mine, 32), :], 10, partner)
    bytes_of(es, 32, recv_sem.at[10])
    for half in range(2):
        for t in range(2):
            rfold[pl.ds(half * 16 + t, 8, stride=2), :] = es[
                pl.ds(half * 32 + c * 2 + t, 8, stride=4), :
            ]
    layer = mixed + rfold[...] + shf[...]
    layer_ref[...] = jnp.concatenate(
        [layer[2 * s : 2 * s + 2] for s in range(16)], axis=1
    ).astype(BF16)

    bytes_of(acts, PLANE - 1, send_sem.at[0])
    bytes_of(wrecv, PLANE - 1, send_sem.at[1])
    bytes_of(qkv_in, PLANE - 1, send_sem.at[2])
    bytes_of(owrecv, PLANE - 1, send_sem.at[3])
    bytes_of(acts2, PLANE - 1, send_sem.at[4])
    bytes_of(oin, PLANE - 1, send_sem.at[5])
    bytes_of(mrecv.at[0], CHIPS - 1, send_sem.at[6])
    bytes_of(mrecv.at[0], CHIPS, send_sem.at[7])
    bytes_of(rpar, SLOTS, send_sem.at[8])
    bytes_of(erecv, CHIPS - 1, send_sem.at[9])
    bytes_of(es, 32, send_sem.at[10])


def on_device(
    hidden_in, lengths, key_cache, value_cache, query_w, key_w, value_w, out_w, lam_heads, head_gain,
    attn_gain, moe_gain, routing, route_weight, gate_w, up_w, down_w, shared_gate, shared_up, shared_down,
):
    inv = (theta_base ** (-np.arange(64, dtype=np.float32) / 64)).astype(np.float32)
    inv = jnp.asarray(np.tile(inv, 2)[None])
    vmem = pl.BlockSpec(memory_space=pltpu.VMEM)
    smem = pl.BlockSpec(memory_space=pltpu.SMEM)
    hbm = pl.BlockSpec(memory_space=pl.ANY)
    V = pltpu.VMEM
    scratch = [
        V((2, 1024, 512), BF16), V((2, 1024, 512), BF16),
        V((D, 512), BF16), V((D, 512), BF16), V((512, D), BF16),
        V((D, 512), BF16), V((D, 512), BF16), V((512, D), BF16),
        V((8, 16, 384), BF16), V((8, 16, 256), BF16), V((32, 16, 384), BF16), V((32, 16, 256), BF16),
        V((32, 128), F32), V((32, 128), F32), V((4, 8, 128), BF16), V((32, 8, 128), BF16),
        V((256, 128), F32), V((256, 128), F32), V((32, 8, 128), F32), V((64, 128), F32),
        V((32, 128), F32), V((4, 8, 128), BF16), V((32, 8, 128), BF16), V((256, 128), F32),
        V((32, 8, 128), F32), V((32, 128), F32),
        V((32, 128), BF16), V((2, 64, 32, 128), BF16), V((4096, 128), F32), V((SLOTS, D), BF16),
        V((2, SLOTS, 1024), BF16), V((SLOTS, 1024), BF16), V((64, 32, 128), BF16), V((64, 32, 128), BF16),
        V((64, 128), F32), V((32, 128), F32), V((32, 128), F32),
        V((2, 256, 128), F32), V((SLOTS, 256), BF16), V((2, 256, 128), F32), V((256, 128), F32),
        pltpu.SemaphoreType.DMA((10,)), pltpu.SemaphoreType.DMA((11,)), pltpu.SemaphoreType.DMA((11,)),
    ]
    return pl.pallas_call(
        kernel,
        out_shape=(
            jax.ShapeDtypeStruct((2, D), BF16),
            jax.ShapeDtypeStruct((2, 512), BF16),
            jax.ShapeDtypeStruct((2, 512), BF16),
        ),
        in_specs=[smem, smem] + [vmem] * 7 + [hbm] * 12,
        out_specs=(vmem, vmem, vmem),
        scratch_shapes=scratch,
        compiler_params=pltpu.CompilerParams(
            collective_id=0, has_side_effects=True, vmem_limit_bytes=56 * 1024 * 1024
        ),
    )(
        lengths, lam_heads, hidden_in, inv,
        attn_gain.reshape(16, 128), moe_gain.reshape(16, 128), head_gain.reshape(1, 256),
        routing, route_weight,
        key_cache, value_cache, query_w, key_w, value_w, out_w, gate_w, up_w, down_w,
        shared_gate, shared_up, shared_down,
    )


def solution(mesh):
    row, cube, whole = P("ep", None), P("ep", None, None), P()
    return jax.shard_map(
        on_device,
        mesh=mesh,
        in_specs=(
            row, P("ep"), cube, cube, row, row, row, row, whole, whole,
            whole, whole, whole, whole, cube, cube, cube, whole, whole, whole,
        ),
        out_specs=(row, row, row),
        check_vma=False,
    )
```

```python
import functools

import jax
import jax.numpy as jnp
import numpy as np
from jax import lax
from jax.experimental import pallas as pl
from jax.experimental.pallas import tpu as pltpu
from jax.sharding import PartitionSpec as P

MESH = pl.DeviceIdType.MESH
F32 = jnp.float32
BF16 = jnp.bfloat16
SIDE = 4
CHIPS = SIDE**3
PLANE = SIDE * SIDE * 2
ISSUE = (2, 1, 3, 0)
ARRIVE = (1, 3, 0, 2)
SLOTS = 32
D = 2048
eps_norm = 1e-06
eps_head = 1e-05
theta_base = 500000.0


def bytes_of(buf, count, sem):
    part = buf.at[pl.ds(0, count)]
    pltpu.make_async_copy(part, part, sem).wait()


def row_parity():
    return lax.broadcasted_iota(jnp.int32, (32, 128), 0) % 2


def fold_rms(fold, gain):
    parity = row_parity()
    squares = fold * fold
    first = jnp.sum(jnp.where(parity == 0, squares, 0.0), keepdims=True)
    second = jnp.sum(jnp.where(parity == 1, squares, 0.0), keepdims=True)
    r0 = lax.rsqrt(first * (1.0 / D) + eps_norm)
    r1 = lax.rsqrt(second * (1.0 / D) + eps_norm)
    return fold * jnp.where(parity == 0, r0, r1) * gain


def kernel(
    len_ref, lam_ref, hidden_ref, inv_ref, again_ref, mgain_ref, hgain_ref, routing_ref, rweight_ref,
    kc_hbm, vc_hbm, qw_hbm, kw_hbm, vw_hbm, ow_hbm, gate_hbm, up_hbm, down_hbm, sg_hbm, su_hbm, sd_hbm,
    layer_ref, kout_ref, vout_ref,
    kc, vc, gate, up, down, sg, su, sd,
    wcat, owcat, wrecv, owrecv,
    hid, gdup, asend, acts, xf, p2, qkv_in, qs,
    af, asend2, acts2, p5, oin, proj,
    ms, mrecv, big, pk, rs, rpar, esend, erecv, es, shf, rfold,
    pt, ptt, wtok, ptmp,
    local_sem, send_sem, recv_sem, ready_sem,
):
    me = lax.axis_index("ep")
    c = me % 2
    p = me // 2
    x = p % SIDE
    y = (p // SIDE) % SIDE
    z = p // (SIDE * SIDE)
    xc = x * 2 + c
    partner = me + 1 - 2 * c
    o_me = z * 8 + xc
    w_me = y * 8 + xc

    def local(src, dst, k):
        cp = pltpu.make_async_copy(src, dst, local_sem.at[k])
        cp.start()
        return cp

    def remote(src, dst, k, target):
        pltpu.make_async_remote_copy(
            src_ref=src,
            dst_ref=dst,
            send_sem=send_sem.at[k],
            recv_sem=recv_sem.at[k],
            device_id=(target,),
            device_id_type=MESH,
        ).start()

    def line_of(k):
        return ((z * SIDE + y) * SIDE + (x + k // 2) % SIDE) * 2 + (c + k % 2) % 2

    barrier = pltpu.get_barrier_semaphore()

    def greet(sem, target):
        pl.semaphore_signal(sem, inc=1, device_id=(target,), device_id_type=MESH)

    for k in range(1, 8):
        greet(barrier, line_of(k))
    for k in range(1, SIDE):
        greet(barrier, ((z * SIDE + (y + k) % SIDE) * SIDE + x) * 2 + c)
        greet(barrier, (((z + k) % SIDE * SIDE + y) * SIDE + x) * 2 + c)

    for h in range(8):
        local(qw_hbm.at[:, pl.ds(h * 256, 256)], wcat.at[h, :, pl.ds(0, 256)], 0)
        kv_hbm = kw_hbm if h < 4 else vw_hbm
        local(kv_hbm.at[:, pl.ds((h % 4) * 128, 128)], wcat.at[h, :, pl.ds(256, 128)], 0)

    wide = hidden_ref[...].astype(F32)
    for s in range(16):
        hid[2 * s : 2 * s + 2, :] = wide[:, 128 * s : 128 * s + 128]
    hidden = hid[...]

    def doubled(gain_ref):
        gdup[pl.ds(0, 16, stride=2), :] = gain_ref[...]
        gdup[pl.ds(1, 16, stride=2), :] = gain_ref[...]
        return gdup[...]

    asend[...] = fold_rms(hidden, doubled(again_ref)).astype(BF16).reshape(4, 8, 128)
    pltpu.make_async_copy(wcat, wcat, local_sem.at[0]).wait()
    for h in range(8):
        local(ow_hbm.at[:, pl.ds(h * 256, 256)], owcat.at[h], 1)
    c_kc = local(kc_hbm, kc, 2)
    c_vc = local(vc_hbm, vc, 3)
    c_sg = local(sg_hbm, sg, 4)
    c_su = local(su_hbm, su, 5)
    c_sd = local(sd_hbm, sd, 6)
    c_gate = local(gate_hbm.at[0], gate, 7)
    c_up = local(up_hbm.at[0], up, 8)
    c_down = local(down_hbm.at[0], down, 9)

    pl.semaphore_wait(barrier, 13)
    for k in range(1, 8):
        greet(ready_sem, line_of(k))
    pl.semaphore_wait(ready_sem, 7)

    def owner_of(k):
        dz, dx, dc = k // 8, (k // 2) % 4, k % 2
        zt, xt, ct = (z + dz) % SIDE, (x + dx) % SIDE, (c + dc) % 2
        return zt, xt * 2 + ct, ((zt * SIDE + y) * SIDE + xt) * 2 + ct

    def holder_of(k):
        dy, dx, dc = k // 8, (k // 2) % 4, k % 2
        yt, xt, ct = (y + dy) % SIDE, (x + dx) % SIDE, (c + dc) % 2
        return xt * 2 + ct, ((z * SIDE + yt) * SIDE + xt) * 2 + ct

    def send_acts(k, _):
        zt, _, target = owner_of(k)
        remote(asend.at[zt], acts.at[o_me], 0, target)
        return 0

    def send_w(k, _):
        ht, target = holder_of(k)
        remote(wcat.at[ht], wrecv.at[w_me], 1, target)
        return 0

    lax.fori_loop(1, PLANE, send_acts, 0)
    lax.fori_loop(1, PLANE, send_w, 0)
    acts[o_me] = asend[z]
    wrecv[w_me] = wcat[xc]

    lane = lax.broadcasted_iota(jnp.int32, (256, 128), 1)
    tri = (
        lax.broadcasted_iota(jnp.int32, (256, 256), 1)
        <= lax.broadcasted_iota(jnp.int32, (256, 256), 0)
    ).astype(BF16)
    for i in range(2):
        expert = me if i == 0 else partner
        match = routing_ref[...] == expert
        here = jnp.max(jnp.where(match, 1.0, 0.0), axis=0, keepdims=True)
        weight = jnp.sum(jnp.where(match, rweight_ref[...], 0.0), axis=0, keepdims=True)
        spread = jnp.transpose(jnp.broadcast_to(here, (128, 256)))
        place = jnp.dot(tri, spread.astype(BF16), preferred_element_type=F32) - 1.0
        table = jnp.where((place == lane.astype(F32)) & (spread > 0.0), 1.0, 0.0)
        ptmp[...] = table
        for ct in range(4):
            pt[i, ct * 64 : ct * 64 + 64, :] = ptmp[pl.ds(ct, 64, stride=4), :]
        ptmp[...] = jnp.transpose(jnp.broadcast_to(weight, (128, 256)))
        for ct in range(4):
            wtok[i, ct * 64 : ct * 64 + 64, :] = ptmp[pl.ds(ct, 64, stride=4), :]
    ptt[...] = jnp.transpose(pt[0])[0:SLOTS].astype(BF16)

    half_sign = jnp.where(lax.broadcasted_iota(jnp.int32, (1, 128), 1) < 64, -1.0, 1.0)
    turns = []
    for t in range(2):
        angle = len_ref[t].astype(F32) * inv_ref[...]
        turns.append((jnp.cos(angle), jnp.sin(angle) * half_sign))

    def columns_of(arrived):
        xf[...] = arrived[...].astype(F32).reshape(256, 128)
        rows = [
            jnp.concatenate(
                [xf[pl.ds(2 * s + t, 32, stride=8), :] for t in range(2)], axis=0
            )
            for s in range(4)
        ]
        return jnp.concatenate(rows, axis=1).astype(BF16)

    bytes_of(acts, PLANE - 1, recv_sem.at[0])
    bytes_of(wrecv, PLANE - 1, recv_sem.at[1])
    part = jnp.dot(
        columns_of(acts), wrecv[...].reshape(512, 384), preferred_element_type=F32
    )
    for b in range(3):
        for t in range(2):
            p2[pl.ds(2 * b + t, 32, stride=8), :] = part[
                32 * t : 32 * t + 32, 128 * b : 128 * b + 128
            ]
    for t in range(2):
        p2[pl.ds(6 + t, 32, stride=8), :] = jnp.zeros((32, 128), F32)

    def send_part(k, _):
        zt, ht, target = owner_of(k)
        ot = pl.multiple_of((zt * 8 + ht) * 8, 8)
        remote(p2.at[pl.ds(ot, 8), :], qkv_in.at[o_me], 2, target)
        return 0

    lax.fori_loop(1, PLANE, send_part, 0)
    qkv_in[o_me] = p2[pl.ds(pl.multiple_of(o_me * 8, 8), 8), :]

    pltpu.make_async_copy(owcat, owcat, local_sem.at[1]).wait()

    def send_ow(k, _):
        ht, target = holder_of(k)
        remote(owcat.at[ht], owrecv.at[w_me], 3, target)
        return 0

    lax.fori_loop(1, PLANE, send_ow, 0)
    owrecv[w_me] = owcat[xc]
    c_kc.wait()
    c_vc.wait()

    bytes_of(qkv_in, PLANE - 1, recv_sem.at[2])
    total = qkv_in[0:8]
    for k in range(1, 4):
        total = total + qkv_in[8 * k : 8 * k + 8]
    qs[...] = total.reshape(64, 128)

    scale = 128.0**-0.5
    row16 = lax.broadcasted_iota(jnp.int32, (16, 128), 0)
    row8 = lax.broadcasted_iota(jnp.int32, (8, 1), 0)
    lam = jnp.zeros((8, 1), F32)
    for h in range(8):
        lam = jnp.where(row8 == h, lam_ref[h], lam)
    keys, values = [], []
    for t in range(2):
        cos, sin = turns[t]

        def turn(v):
            return v * cos + pltpu.roll(v, 64, 1) * sin

        kv = qs[pl.ds(4 + t, 8, stride=8), :]
        q16 = jnp.concatenate(
            [turn(qs[pl.ds(t, 8, stride=8), :]), turn(qs[pl.ds(2 + t, 8, stride=8), :])],
            axis=0,
        )
        q16 = q16.astype(BF16).astype(F32)
        kn = turn(kv).astype(BF16).astype(F32)
        vn = kv.astype(BF16).astype(F32)
        keys.append(jnp.concatenate([kn[i : i + 1] for i in range(4)], axis=1))
        vflat = jnp.concatenate([vn[i : i + 1] for i in range(4, 8)], axis=1)
        values.append(vflat)
        own_keys = jnp.concatenate(
            [jnp.broadcast_to(kn[i : i + 1], (4, 128)) for i in (0, 2, 1, 3)], axis=0
        )
        self_score = jnp.sum(q16 * own_keys, axis=1, keepdims=True) * scale
        blocks = []
        for k in range(2):
            for j in range(2):
                lo = j * 8 + k * 4
                blocks.append(jnp.where((row16 >= lo) & (row16 < lo + 4), q16, 0.0))
        wide_q = jnp.concatenate(blocks, axis=1).astype(BF16)
        scores = (
            lax.dot_general(
                wide_q, kc[t], (((1,), (1,)), ((), ())), preferred_element_type=F32
            )
            * scale
        )
        live = lax.broadcasted_iota(jnp.int32, (16, 1024), 1) < len_ref[t]
        peak = jnp.maximum(
            jnp.max(jnp.where(live, scores, -jnp.inf), axis=1, keepdims=True), self_score
        )
        weights = jnp.where(live, jnp.exp(scores - peak), 0.0)
        self_w = jnp.exp(self_score - peak)
        totals = jnp.sum(weights, axis=1, keepdims=True) + self_w
        comb = weights[0:8] / totals[0:8] - lam * weights[8:16] / totals[8:16]
        self_comb = self_w[0:8] / totals[0:8] - lam * self_w[8:16] / totals[8:16]
        out = jnp.dot(comb.astype(BF16), vc[t], preferred_element_type=F32)
        out = out + self_comb.astype(BF16).astype(F32) * vflat
        head = jnp.where(row8 < 4, out[:, 0:256], out[:, 256:512])
        mean = jnp.sum(head * head, axis=1, keepdims=True) * (1.0 / 256)
        head = head * lax.rsqrt(mean + eps_head) * hgain_ref[...]
        for half in range(2):
            af[pl.ds(2 * half + t, 8, stride=4), :] = head[:, 128 * half : 128 * half + 128]
    kout_ref[...] = jnp.concatenate(keys, axis=0).astype(BF16)
    vout_ref[...] = jnp.concatenate(values, axis=0).astype(BF16)
    asend2[...] = af[...].astype(BF16).reshape(4, 8, 128)

    def send_acts2(k, _):
        zt, _, target = owner_of(k)
        remote(asend2.at[zt], acts2.at[o_me], 4, target)
        return 0

    lax.fori_loop(1, PLANE, send_acts2, 0)
    acts2[o_me] = asend2[z]
    mgain = doubled(mgain_ref)
    bytes_of(owrecv, PLANE - 1, recv_sem.at[3])
    bytes_of(acts2, PLANE - 1, recv_sem.at[4])
    part = jnp.dot(
        columns_of(acts2), owrecv[...].reshape(512, 256), preferred_element_type=F32
    )
    for b in range(2):
        for t in range(2):
            p5[pl.ds(2 * b + t, 32, stride=8), :] = part[
                32 * t : 32 * t + 32, 128 * b : 128 * b + 128
            ]
    for r in range(4, 8):
        p5[pl.ds(r, 32, stride=8), :] = jnp.zeros((32, 128), F32)

    def send_part2(k, _):
        zt, ht, target = owner_of(k)
        ot = pl.multiple_of((zt * 8 + ht) * 8, 8)
        remote(p5.at[pl.ds(ot, 8), :], oin.at[o_me], 5, target)
        return 0

    lax.fori_loop(1, PLANE, send_part2, 0)
    oin[o_me] = p5[pl.ds(pl.multiple_of(o_me * 8, 8), 8), :]
    bytes_of(oin, PLANE - 1, recv_sem.at[5])
    total = oin[0:8]
    for k in range(1, 4):
        total = total + oin[8 * k : 8 * k + 8]
    for h in range(8):
        proj[4 * h : 4 * h + 4, :] = total[h, 0:4]
    mixed = (hidden + proj[...].astype(BF16).astype(F32)).astype(BF16).astype(F32)
    moe = fold_rms(mixed, mgain).astype(BF16)
    ms[...] = moe

    def chip_at(dz, k):
        zt, yt, xt = (z + dz) % SIDE, (y + k // SIDE) % SIDE, (x + k % SIDE) % SIDE
        return (zt * SIDE + yt) * SIDE + xt

    def group(dz):
        return pl.multiple_of((z - dz + SIDE) % SIDE * 16, 16), 16 if dz else 15

    for dz in ISSUE:

        def send_moe(k, _, dz=dz):
            remote(ms, mrecv.at[c, p], 12 + dz, chip_at(dz, k) * 2 + c)
            return 0

        lax.fori_loop(0 if dz else 1, 16, send_moe, 0)
    mrecv[c, p] = moe

    moe32 = moe.astype(F32)
    lhs = jnp.concatenate([moe32[2 * s : 2 * s + 2] for s in range(16)], axis=1).astype(BF16)
    c_sg.wait()
    c_su.wait()
    c_sd.wait()
    g = jnp.dot(lhs, sg[...], preferred_element_type=F32)
    u = jnp.dot(lhs, su[...], preferred_element_type=F32)
    shared = jnp.dot(
        (jax.nn.silu(g) * u).astype(BF16), sd[...], preferred_element_type=F32
    )
    for s in range(16):
        shf[2 * s : 2 * s + 2, :] = shared[:, 128 * s : 128 * s + 128]
    c_gate.wait()
    c_up.wait()
    c_down.wait()

    def widen(core, first):
        for i in range(4):
            start = pl.multiple_of(core * 2048 + (first + 4 * i) * 32, 128)
            big[pl.ds(start, 128), :] = (
                mrecv[core, pl.ds(first + 4 * i, 4)].astype(F32).reshape(128, 128)
            )

    for dz in ARRIVE:
        first, count = group(dz)
        bytes_of(mrecv.at[0], count, recv_sem.at[12 + dz])
        block = mrecv.at[c, pl.ds(first, 16)]
        remote(block, block, 16 + dz, partner)
        widen(c, first)
    for dz in ARRIVE:
        first, _ = group(dz)
        bytes_of(mrecv.at[0], 16, recv_sem.at[16 + dz])
        widen(1 - c, first)
    for s in range(16):
        rows = jnp.concatenate(
            [
                big[pl.ds((ct // 2) * 2048 + 2 * s + ct % 2, 64, stride=32), :]
                for ct in range(4)
            ],
            axis=0,
        ).astype(BF16)
        pk[:, 128 * s : 128 * s + 128] = jnp.dot(
            ptt[...], rows, preferred_element_type=F32
        ).astype(BF16)
    g = jnp.dot(pk[...], gate[...], preferred_element_type=F32)
    u = jnp.dot(pk[...], up[...], preferred_element_type=F32)
    hidden_e = (jax.nn.silu(g) * u).astype(BF16)
    for i in range(2):
        rs[i] = jnp.dot(
            hidden_e, down[:, 1024 * i : 1024 * i + 1024], preferred_element_type=F32
        ).astype(BF16)

    remote(rs.at[1 - c], rpar, 8, partner)
    own = jnp.dot(pt[0, :, 0:SLOTS].astype(BF16), rs[c], preferred_element_type=F32)
    for ct in range(4):
        for s in range(8):
            big[pl.ds(4 * s + ct, 64, stride=32), :] = (
                own[64 * ct : 64 * ct + 64, 128 * s : 128 * s + 128]
                * wtok[0, 64 * ct : 64 * ct + 64, :]
            )
    bytes_of(rpar, SLOTS, recv_sem.at[8])
    other = jnp.dot(pt[1, :, 0:SLOTS].astype(BF16), rpar[...], preferred_element_type=F32)
    for ct in range(4):
        for s in range(8):
            big[pl.ds(4 * s + ct, 64, stride=32), :] = (
                big[pl.ds(4 * s + ct, 64, stride=32), :]
                + other[64 * ct : 64 * ct + 64, 128 * s : 128 * s + 128]
                * wtok[1, 64 * ct : 64 * ct + 64, :]
            )

    for dz in ISSUE:
        start = (z + dz) % SIDE * 16
        for i in range(4):
            rows = pl.multiple_of((start + 4 * i) * 32, 128)
            esend[pl.ds(start + 4 * i, 4)] = (
                big[pl.ds(rows, 128), :].astype(BF16).reshape(4, 32, 128)
            )

        def send_back(k, _, dz=dz):
            chip = chip_at(dz, k)
            remote(esend.at[chip], erecv.at[p], 20 + dz, chip * 2 + c)
            return 0

        lax.fori_loop(0 if dz else 1, 16, send_back, 0)
    erecv[p] = esend[p]
    total = jnp.zeros((32, 128), F32)
    for dz in ARRIVE:
        first, count = group(dz)
        bytes_of(erecv, count, recv_sem.at[20 + dz])
        for i in range(4):
            total = total + jnp.sum(erecv[pl.ds(first + 4 * i, 4)].astype(F32), axis=0)
    mine = pl.multiple_of(c * 32, 32)
    es[pl.ds(mine, 32), :] = total
    remote(es.at[pl.ds(mine, 32), :], es.at[pl.ds(mine, 32), :], 10, partner)
    bytes_of(es, 32, recv_sem.at[10])
    for half in range(2):
        for t in range(2):
            rfold[pl.ds(half * 16 + t, 8, stride=2), :] = es[
                pl.ds(half * 32 + c * 2 + t, 8, stride=4), :
            ]
    layer = mixed + rfold[...] + shf[...]
    layer_ref[...] = jnp.concatenate(
        [layer[2 * s : 2 * s + 2] for s in range(16)], axis=1
    ).astype(BF16)

    bytes_of(acts, PLANE - 1, send_sem.at[0])
    bytes_of(wrecv, PLANE - 1, send_sem.at[1])
    bytes_of(qkv_in, PLANE - 1, send_sem.at[2])
    bytes_of(owrecv, PLANE - 1, send_sem.at[3])
    bytes_of(acts2, PLANE - 1, send_sem.at[4])
    bytes_of(oin, PLANE - 1, send_sem.at[5])
    bytes_of(rpar, SLOTS, send_sem.at[8])
    bytes_of(es, 32, send_sem.at[10])
    for dz in range(SIDE):
        count = 16 if dz else 15
        bytes_of(mrecv.at[0], count, send_sem.at[12 + dz])
        bytes_of(mrecv.at[0], 16, send_sem.at[16 + dz])
        bytes_of(erecv, count, send_sem.at[20 + dz])


def hand_over(*refs):
    for i in range(3):
        refs[3 + i][...] = refs[i][...]


def on_device(
    hidden_in, lengths, key_cache, value_cache, query_w, key_w, value_w, out_w, lam_heads, head_gain,
    attn_gain, moe_gain, routing, route_weight, gate_w, up_w, down_w, shared_gate, shared_up, shared_down,
):
    inv = (theta_base ** (-np.arange(64, dtype=np.float32) / 64)).astype(np.float32)
    inv = jnp.asarray(np.tile(inv, 2)[None])
    vmem = pl.BlockSpec(memory_space=pltpu.VMEM)
    smem = pl.BlockSpec(memory_space=pltpu.SMEM)
    hbm = pl.BlockSpec(memory_space=pl.ANY)
    V = pltpu.VMEM
    scratch = [
        V((2, 1024, 512), BF16), V((2, 1024, 512), BF16),
        V((D, 512), BF16), V((D, 512), BF16), V((512, D), BF16),
        V((D, 512), BF16), V((D, 512), BF16), V((512, D), BF16),
        V((8, 16, 384), BF16), V((8, 16, 256), BF16), V((32, 16, 384), BF16), V((32, 16, 256), BF16),
        V((32, 128), F32), V((32, 128), F32), V((4, 8, 128), BF16), V((32, 8, 128), BF16),
        V((256, 128), F32), V((256, 128), F32), V((32, 8, 128), F32), V((64, 128), F32),
        V((32, 128), F32), V((4, 8, 128), BF16), V((32, 8, 128), BF16), V((256, 128), F32),
        V((32, 8, 128), F32), V((32, 128), F32),
        V((32, 128), BF16), V((2, 64, 32, 128), BF16), V((4096, 128), F32), V((SLOTS, D), BF16),
        V((2, SLOTS, 1024), BF16), V((SLOTS, 1024), BF16), V((64, 32, 128), BF16), V((64, 32, 128), BF16),
        V((64, 128), F32), V((32, 128), F32), V((32, 128), F32),
        V((2, 256, 128), F32), V((SLOTS, 256), BF16), V((2, 256, 128), F32), V((256, 128), F32),
        pltpu.SemaphoreType.DMA((10,)), pltpu.SemaphoreType.DMA((24,)), pltpu.SemaphoreType.DMA((24,)),
        pltpu.SemaphoreType.REGULAR,
    ]
    shapes = (
        jax.ShapeDtypeStruct((2, D), BF16),
        jax.ShapeDtypeStruct((2, 512), BF16),
        jax.ShapeDtypeStruct((2, 512), BF16),
    )
    results = pl.pallas_call(
        kernel,
        out_shape=shapes,
        in_specs=[smem, smem] + [vmem] * 7 + [hbm] * 12,
        out_specs=(vmem, vmem, vmem),
        scratch_shapes=scratch,
        compiler_params=pltpu.CompilerParams(
            collective_id=0, has_side_effects=True, vmem_limit_bytes=56 * 1024 * 1024
        ),
    )(
        lengths, lam_heads, hidden_in, inv,
        attn_gain.reshape(16, 128), moe_gain.reshape(16, 128), head_gain.reshape(1, 256),
        routing.T, route_weight.T,
        key_cache, value_cache, query_w, key_w, value_w, out_w, gate_w, up_w, down_w,
        shared_gate, shared_up, shared_down,
    )
    return pl.pallas_call(
        hand_over, out_shape=shapes, in_specs=[vmem] * 3, out_specs=(vmem,) * 3
    )(*results)


def solution(mesh):
    row, cube, whole = P("ep", None), P("ep", None, None), P()
    return jax.shard_map(
        on_device,
        mesh=mesh,
        in_specs=(
            row, P("ep"), cube, cube, row, row, row, row, whole, whole,
            whole, whole, whole, whole, cube, cube, cube, whole, whole, whole,
        ),
        out_specs=(row, row, row),
        check_vma=False,
    )
```

```python
import functools

import jax
import jax.numpy as jnp
import numpy as np
from jax import lax
from jax.experimental import pallas as pl
from jax.experimental.pallas import tpu as pltpu
from jax.sharding import PartitionSpec as P

MESH = pl.DeviceIdType.MESH
F32 = jnp.float32
BF16 = jnp.bfloat16
SIDE = 4
CHIPS = SIDE**3
PLANE = SIDE * SIDE * 2
ISSUE = (2, 1, 3, 0)
ARRIVE = (1, 3, 0, 2)
SLOTS = 32
D = 2048
eps_norm = 1e-06
eps_head = 1e-05
theta_base = 500000.0


def bytes_of(buf, count, sem):
    part = buf.at[pl.ds(0, count)]
    pltpu.make_async_copy(part, part, sem).wait()


def row_parity():
    return lax.broadcasted_iota(jnp.int32, (32, 128), 0) % 2


def fold_rms(fold, gain):
    parity = row_parity()
    squares = fold * fold
    first = jnp.sum(jnp.where(parity == 0, squares, 0.0), keepdims=True)
    second = jnp.sum(jnp.where(parity == 1, squares, 0.0), keepdims=True)
    r0 = lax.rsqrt(first * (1.0 / D) + eps_norm)
    r1 = lax.rsqrt(second * (1.0 / D) + eps_norm)
    return fold * jnp.where(parity == 0, r0, r1) * gain


def kernel(
    len_ref, lam_ref, hidden_ref, inv_ref, again_ref, mgain_ref, hgain_ref, routing_ref, rweight_ref,
    kc_hbm, vc_hbm, qw_hbm, kw_hbm, vw_hbm, ow_hbm, gate_hbm, up_hbm, down_hbm, sg_hbm, su_hbm, sd_hbm,
    layer_ref, kout_ref, vout_ref,
    kc, vc, gate, up, down, sg, su, sd,
    wcat, owcat, wrecv, owrecv,
    hid, gdup, asend, acts, xf, p2, qkv_in, qs,
    af, asend2, acts2, p5, oin, proj,
    ms, mrecv, big, pk, pgive, ptake, rs, rpar, esend, erecv, shf,
    pt, ptt, ptmp,
    local_sem, send_sem, recv_sem, ready_sem,
):
    me = lax.axis_index("ep")
    c = me % 2
    p = me // 2
    x = p % SIDE
    y = (p // SIDE) % SIDE
    z = p // (SIDE * SIDE)
    xc = x * 2 + c
    partner = me + 1 - 2 * c
    o_me = z * 8 + xc
    w_me = y * 8 + xc

    def local(src, dst, k):
        cp = pltpu.make_async_copy(src, dst, local_sem.at[k])
        cp.start()
        return cp

    def remote(src, dst, k, target):
        pltpu.make_async_remote_copy(
            src_ref=src,
            dst_ref=dst,
            send_sem=send_sem.at[k],
            recv_sem=recv_sem.at[k],
            device_id=(target,),
            device_id_type=MESH,
        ).start()

    def line_of(k):
        return ((z * SIDE + y) * SIDE + (x + k // 2) % SIDE) * 2 + (c + k % 2) % 2

    barrier = pltpu.get_barrier_semaphore()

    def greet(sem, target):
        pl.semaphore_signal(sem, inc=1, device_id=(target,), device_id_type=MESH)

    for k in range(1, 8):
        greet(barrier, line_of(k))
    for k in range(1, SIDE):
        greet(barrier, ((z * SIDE + (y + k) % SIDE) * SIDE + x) * 2 + c)
        greet(barrier, (((z + k) % SIDE * SIDE + y) * SIDE + x) * 2 + c)

    for h in range(8):
        local(qw_hbm.at[:, pl.ds(h * 256, 256)], wcat.at[h, :, pl.ds(0, 256)], 0)
        kv_hbm = kw_hbm if h < 4 else vw_hbm
        local(kv_hbm.at[:, pl.ds((h % 4) * 128, 128)], wcat.at[h, :, pl.ds(256, 128)], 0)

    wide = hidden_ref[...].astype(F32)
    for s in range(16):
        hid[2 * s : 2 * s + 2, :] = wide[:, 128 * s : 128 * s + 128]
    hidden = hid[...]

    def doubled(gain_ref):
        gdup[pl.ds(0, 16, stride=2), :] = gain_ref[...]
        gdup[pl.ds(1, 16, stride=2), :] = gain_ref[...]
        return gdup[...]

    asend[...] = fold_rms(hidden, doubled(again_ref)).astype(BF16).reshape(4, 8, 128)
    pltpu.make_async_copy(wcat, wcat, local_sem.at[0]).wait()
    for h in range(8):
        local(ow_hbm.at[:, pl.ds(h * 256, 256)], owcat.at[h], 1)
    c_kc = local(kc_hbm, kc, 2)
    c_vc = local(vc_hbm, vc, 3)
    c_sg = local(sg_hbm, sg, 4)
    c_su = local(su_hbm, su, 5)
    c_sd = local(sd_hbm, sd, 6)
    c_gate = local(gate_hbm.at[0], gate, 7)
    c_up = local(up_hbm.at[0], up, 8)
    c_down = local(down_hbm.at[0], down, 9)

    pl.semaphore_wait(barrier, 13)
    for k in range(1, 8):
        greet(ready_sem, line_of(k))
    pl.semaphore_wait(ready_sem, 7)

    def owner_of(k):
        dz, dx, dc = k // 8, (k // 2) % 4, k % 2
        zt, xt, ct = (z + dz) % SIDE, (x + dx) % SIDE, (c + dc) % 2
        return zt, xt * 2 + ct, ((zt * SIDE + y) * SIDE + xt) * 2 + ct

    def holder_of(k):
        dy, dx, dc = k // 8, (k // 2) % 4, k % 2
        yt, xt, ct = (y + dy) % SIDE, (x + dx) % SIDE, (c + dc) % 2
        return xt * 2 + ct, ((z * SIDE + yt) * SIDE + xt) * 2 + ct

    def send_acts(k, _):
        zt, _, target = owner_of(k)
        remote(asend.at[zt], acts.at[o_me], 0, target)
        return 0

    def send_w(k, _):
        ht, target = holder_of(k)
        remote(wcat.at[ht], wrecv.at[w_me], 1, target)
        return 0

    lax.fori_loop(1, PLANE, send_acts, 0)
    lax.fori_loop(1, PLANE, send_w, 0)
    acts[o_me] = asend[z]
    wrecv[w_me] = wcat[xc]

    upto = (
        lax.broadcasted_iota(jnp.int32, (256, 256), 0)
        <= lax.broadcasted_iota(jnp.int32, (256, 256), 1)
    ).astype(BF16)
    slot = lax.broadcasted_iota(jnp.int32, (SLOTS, 256), 0).astype(F32)
    tables = []
    for expert in (me, partner):
        match = routing_ref[...] == expert
        here = jnp.max(jnp.where(match, 1.0, 0.0), axis=0, keepdims=True)
        rows = jnp.broadcast_to(here, (8, 256)).astype(BF16)
        place = jnp.dot(rows, upto, preferred_element_type=F32)[0:1] - 1.0
        tables.append(jnp.where((place == slot) & (here > 0.0), 1.0, 0.0))
        if expert is me:
            weight = jnp.sum(jnp.where(match, rweight_ref[...], 0.0), axis=0, keepdims=True)
            slot_w = jnp.sum(tables[0] * weight, axis=1, keepdims=True)
    tables.append(jnp.zeros((128 - 2 * SLOTS, 256), F32))
    ptmp[...] = jnp.transpose(jnp.concatenate(tables, axis=0))
    for zq in range(SIDE):
        for ct in range(4):
            at = zq * 64 + ct * 16
            pt[at : at + 16, :] = ptmp[pl.ds(zq * 64 + ct, 16, stride=4), :]
    seen = jnp.concatenate(
        [ptmp[pl.ds(c * 2 + t, 64, stride=4), :] for t in range(2)], axis=0
    )
    ptt[...] = jnp.transpose(seen)[0 : 2 * SLOTS].astype(BF16)

    half_sign = jnp.where(lax.broadcasted_iota(jnp.int32, (1, 128), 1) < 64, -1.0, 1.0)
    turns = []
    for t in range(2):
        angle = len_ref[t].astype(F32) * inv_ref[...]
        turns.append((jnp.cos(angle), jnp.sin(angle) * half_sign))

    def columns_of(arrived):
        xf[...] = arrived[...].astype(F32).reshape(256, 128)
        rows = [
            jnp.concatenate(
                [xf[pl.ds(2 * s + t, 32, stride=8), :] for t in range(2)], axis=0
            )
            for s in range(4)
        ]
        return jnp.concatenate(rows, axis=1).astype(BF16)

    bytes_of(acts, PLANE - 1, recv_sem.at[0])
    bytes_of(wrecv, PLANE - 1, recv_sem.at[1])
    part = jnp.dot(
        columns_of(acts), wrecv[...].reshape(512, 384), preferred_element_type=F32
    )
    for b in range(3):
        for t in range(2):
            p2[pl.ds(2 * b + t, 32, stride=8), :] = part[
                32 * t : 32 * t + 32, 128 * b : 128 * b + 128
            ]
    for t in range(2):
        p2[pl.ds(6 + t, 32, stride=8), :] = jnp.zeros((32, 128), F32)

    def send_part(k, _):
        zt, ht, target = owner_of(k)
        ot = pl.multiple_of((zt * 8 + ht) * 8, 8)
        remote(p2.at[pl.ds(ot, 8), :], qkv_in.at[o_me], 2, target)
        return 0

    lax.fori_loop(1, PLANE, send_part, 0)
    qkv_in[o_me] = p2[pl.ds(pl.multiple_of(o_me * 8, 8), 8), :]

    pltpu.make_async_copy(owcat, owcat, local_sem.at[1]).wait()

    def send_ow(k, _):
        ht, target = holder_of(k)
        remote(owcat.at[ht], owrecv.at[w_me], 3, target)
        return 0

    lax.fori_loop(1, PLANE, send_ow, 0)
    owrecv[w_me] = owcat[xc]
    c_kc.wait()
    c_vc.wait()

    bytes_of(qkv_in, PLANE - 1, recv_sem.at[2])
    total = qkv_in[0:8]
    for k in range(1, 4):
        total = total + qkv_in[8 * k : 8 * k + 8]
    qs[...] = total.reshape(64, 128)

    scale = 128.0**-0.5
    row16 = lax.broadcasted_iota(jnp.int32, (16, 128), 0)
    row8 = lax.broadcasted_iota(jnp.int32, (8, 1), 0)
    lam = jnp.zeros((8, 1), F32)
    for h in range(8):
        lam = jnp.where(row8 == h, lam_ref[h], lam)
    keys, values = [], []
    for t in range(2):
        cos, sin = turns[t]

        def turn(v):
            return v * cos + pltpu.roll(v, 64, 1) * sin

        kv = qs[pl.ds(4 + t, 8, stride=8), :]
        q16 = jnp.concatenate(
            [turn(qs[pl.ds(t, 8, stride=8), :]), turn(qs[pl.ds(2 + t, 8, stride=8), :])],
            axis=0,
        )
        q16 = q16.astype(BF16).astype(F32)
        kn = turn(kv).astype(BF16).astype(F32)
        vn = kv.astype(BF16).astype(F32)
        keys.append(jnp.concatenate([kn[i : i + 1] for i in range(4)], axis=1))
        vflat = jnp.concatenate([vn[i : i + 1] for i in range(4, 8)], axis=1)
        values.append(vflat)
        own_keys = jnp.concatenate(
            [jnp.broadcast_to(kn[i : i + 1], (4, 128)) for i in (0, 2, 1, 3)], axis=0
        )
        self_score = jnp.sum(q16 * own_keys, axis=1, keepdims=True) * scale
        blocks = []
        for k in range(2):
            for j in range(2):
                lo = j * 8 + k * 4
                blocks.append(jnp.where((row16 >= lo) & (row16 < lo + 4), q16, 0.0))
        wide_q = jnp.concatenate(blocks, axis=1).astype(BF16)
        scores = (
            lax.dot_general(
                wide_q, kc[t], (((1,), (1,)), ((), ())), preferred_element_type=F32
            )
            * scale
        )
        live = lax.broadcasted_iota(jnp.int32, (16, 1024), 1) < len_ref[t]
        peak = jnp.maximum(
            jnp.max(jnp.where(live, scores, -jnp.inf), axis=1, keepdims=True), self_score
        )
        weights = jnp.where(live, jnp.exp(scores - peak), 0.0)
        self_w = jnp.exp(self_score - peak)
        totals = jnp.sum(weights, axis=1, keepdims=True) + self_w
        comb = weights[0:8] / totals[0:8] - lam * weights[8:16] / totals[8:16]
        self_comb = self_w[0:8] / totals[0:8] - lam * self_w[8:16] / totals[8:16]
        out = jnp.dot(comb.astype(BF16), vc[t], preferred_element_type=F32)
        out = out + self_comb.astype(BF16).astype(F32) * vflat
        head = jnp.where(row8 < 4, out[:, 0:256], out[:, 256:512])
        mean = jnp.sum(head * head, axis=1, keepdims=True) * (1.0 / 256)
        head = head * lax.rsqrt(mean + eps_head) * hgain_ref[...]
        for half in range(2):
            af[pl.ds(2 * half + t, 8, stride=4), :] = head[:, 128 * half : 128 * half + 128]
    kout_ref[...] = jnp.concatenate(keys, axis=0).astype(BF16)
    vout_ref[...] = jnp.concatenate(values, axis=0).astype(BF16)
    asend2[...] = af[...].astype(BF16).reshape(4, 8, 128)

    def send_acts2(k, _):
        zt, _, target = owner_of(k)
        remote(asend2.at[zt], acts2.at[o_me], 4, target)
        return 0

    lax.fori_loop(1, PLANE, send_acts2, 0)
    acts2[o_me] = asend2[z]
    mgain = doubled(mgain_ref)
    bytes_of(owrecv, PLANE - 1, recv_sem.at[3])
    bytes_of(acts2, PLANE - 1, recv_sem.at[4])
    part = jnp.dot(
        columns_of(acts2), owrecv[...].reshape(512, 256), preferred_element_type=F32
    )
    for b in range(2):
        for t in range(2):
            p5[pl.ds(2 * b + t, 32, stride=8), :] = part[
                32 * t : 32 * t + 32, 128 * b : 128 * b + 128
            ]
    for r in range(4, 8):
        p5[pl.ds(r, 32, stride=8), :] = jnp.zeros((32, 128), F32)

    def send_part2(k, _):
        zt, ht, target = owner_of(k)
        ot = pl.multiple_of((zt * 8 + ht) * 8, 8)
        remote(p5.at[pl.ds(ot, 8), :], oin.at[o_me], 5, target)
        return 0

    lax.fori_loop(1, PLANE, send_part2, 0)
    oin[o_me] = p5[pl.ds(pl.multiple_of(o_me * 8, 8), 8), :]
    bytes_of(oin, PLANE - 1, recv_sem.at[5])
    total = oin[0:8]
    for k in range(1, 4):
        total = total + oin[8 * k : 8 * k + 8]
    for h in range(8):
        proj[4 * h : 4 * h + 4, :] = total[h, 0:4]
    mixed = (hidden + proj[...].astype(BF16).astype(F32)).astype(BF16).astype(F32)
    moe = fold_rms(mixed, mgain).astype(BF16)
    ms[...] = moe

    def chip_at(dz, k):
        zt, yt, xt = (z + dz) % SIDE, (y + k // SIDE) % SIDE, (x + k % SIDE) % SIDE
        return (zt * SIDE + yt) * SIDE + xt

    def group(dz):
        return pl.multiple_of((z - dz + SIDE) % SIDE * 16, 16), 16 if dz else 15

    for dz in ISSUE:

        def send_moe(k, _, dz=dz):
            remote(ms, mrecv.at[p], 12 + dz, chip_at(dz, k) * 2 + c)
            return 0

        lax.fori_loop(0 if dz else 1, 16, send_moe, 0)
    mrecv[p] = moe

    moe32 = moe.astype(F32)
    lhs = jnp.concatenate([moe32[2 * s : 2 * s + 2] for s in range(16)], axis=1).astype(BF16)
    c_sg.wait()
    c_su.wait()
    c_sd.wait()
    g = jnp.dot(lhs, sg[...], preferred_element_type=F32)
    u = jnp.dot(lhs, su[...], preferred_element_type=F32)
    shared = jnp.dot(
        (jax.nn.silu(g) * u).astype(BF16), sd[...], preferred_element_type=F32
    )
    for s in range(16):
        shf[2 * s : 2 * s + 2, :] = shared[:, 128 * s : 128 * s + 128]
    c_gate.wait()
    c_up.wait()
    c_down.wait()

    for dz in ARRIVE:
        first, count = group(dz)
        bytes_of(mrecv, count, recv_sem.at[12 + dz])
        for i in range(4):
            start = pl.multiple_of((first + 4 * i) * 32, 128)
            big[pl.ds(start, 128), :] = (
                mrecv[pl.ds(first + 4 * i, 4)].astype(F32).reshape(128, 128)
            )
    for s in range(8):
        rows = jnp.concatenate(
            [
                jnp.concatenate(
                    [big[pl.ds(4 * s + 2 * i + t, 64, stride=32), :] for t in range(2)], axis=0
                )
                for i in range(2)
            ],
            axis=1,
        ).astype(BF16)
        picked = jnp.dot(ptt[...], rows, preferred_element_type=F32).astype(BF16)
        pk[:, 256 * s : 256 * s + 256] = picked[0:SLOTS]
        pgive[:, 256 * s : 256 * s + 256] = picked[SLOTS : 2 * SLOTS]
    remote(pgive, ptake, 7, partner)
    bytes_of(ptake, SLOTS, recv_sem.at[7])
    pk[...] = (pk[...].astype(F32) + ptake[...].astype(F32)).astype(BF16)
    g = jnp.dot(pk[...], gate[...], preferred_element_type=F32)
    u = jnp.dot(pk[...], up[...], preferred_element_type=F32)
    hidden_e = (jax.nn.silu(g) * u).astype(BF16)
    for i in range(2):
        made = jnp.dot(
            hidden_e, down[:, 1024 * i : 1024 * i + 1024], preferred_element_type=F32
        ).astype(BF16)
        rs[i] = (made.astype(F32) * slot_w).astype(BF16)

    remote(rs.at[1 - c], rpar, 8, partner)
    bytes_of(rpar, SLOTS, recv_sem.at[8])
    pair = jnp.concatenate([rs[c], rpar[...]], axis=0)
    for dz in ISSUE:
        zt = (z + dz) % SIDE
        rows = pt[pl.ds(pl.multiple_of(zt * 64, 64), 64), 0 : 2 * SLOTS].astype(BF16)
        both = jnp.dot(rows, pair, preferred_element_type=F32)
        for ct in range(4):
            for s in range(8):
                big[pl.ds(dz * 512 + (ct // 2) * 16 + 2 * s + ct % 2, 16, stride=32), :] = both[
                    16 * ct : 16 * ct + 16, 128 * s : 128 * s + 128
                ]
        for i in range(4):
            at = dz * 512 + i * 128
            esend[pl.ds((zt * 16 + 4 * i) * 2, 8)] = (
                big[at : at + 128, :].astype(BF16).reshape(8, 16, 128)
            )

        def send_back(k, _, dz=dz):
            chip, core = chip_at(dz, k // 2), (c + k % 2) % 2
            device = chip * 2 + core
            remote(esend.at[device], erecv.at[c * CHIPS + p], 20 + dz, device)
            return 0

        lax.fori_loop(0 if dz else 1, 32, send_back, 0)
    erecv[c * CHIPS + p] = esend[me]
    halves = [jnp.zeros((16, 128), F32)] * 2
    for dz in ARRIVE:
        first, count = group(dz)
        bytes_of(erecv, 16 + count, recv_sem.at[20 + dz])
        for half in range(2):
            for i in range(2):
                rows = erecv[pl.ds(half * CHIPS + first + 8 * i, 8)].astype(F32)
                halves[half] = halves[half] + jnp.sum(rows, axis=0)
    routed = jnp.concatenate(halves, axis=0)
    layer = mixed + routed + shf[...]
    layer_ref[...] = jnp.concatenate(
        [layer[2 * s : 2 * s + 2] for s in range(16)], axis=1
    ).astype(BF16)

    bytes_of(acts, PLANE - 1, send_sem.at[0])
    bytes_of(wrecv, PLANE - 1, send_sem.at[1])
    bytes_of(qkv_in, PLANE - 1, send_sem.at[2])
    bytes_of(owrecv, PLANE - 1, send_sem.at[3])
    bytes_of(acts2, PLANE - 1, send_sem.at[4])
    bytes_of(oin, PLANE - 1, send_sem.at[5])
    bytes_of(ptake, SLOTS, send_sem.at[7])
    bytes_of(rpar, SLOTS, send_sem.at[8])
    for dz in range(SIDE):
        count = 16 if dz else 15
        bytes_of(mrecv, count, send_sem.at[12 + dz])
        bytes_of(erecv, 16 + count, send_sem.at[20 + dz])


def hand_over(*refs):
    for i in range(3):
        refs[3 + i][...] = refs[i][...]


def on_device(
    hidden_in, lengths, key_cache, value_cache, query_w, key_w, value_w, out_w, lam_heads, head_gain,
    attn_gain, moe_gain, routing, route_weight, gate_w, up_w, down_w, shared_gate, shared_up, shared_down,
):
    inv = (theta_base ** (-np.arange(64, dtype=np.float32) / 64)).astype(np.float32)
    inv = jnp.asarray(np.tile(inv, 2)[None])
    vmem = pl.BlockSpec(memory_space=pltpu.VMEM)
    smem = pl.BlockSpec(memory_space=pltpu.SMEM)
    hbm = pl.BlockSpec(memory_space=pl.ANY)
    V = pltpu.VMEM
    scratch = [
        V((2, 1024, 512), BF16), V((2, 1024, 512), BF16),
        V((D, 512), BF16), V((D, 512), BF16), V((512, D), BF16),
        V((D, 512), BF16), V((D, 512), BF16), V((512, D), BF16),
        V((8, 16, 384), BF16), V((8, 16, 256), BF16), V((32, 16, 384), BF16), V((32, 16, 256), BF16),
        V((32, 128), F32), V((32, 128), F32), V((4, 8, 128), BF16), V((32, 8, 128), BF16),
        V((256, 128), F32), V((256, 128), F32), V((32, 8, 128), F32), V((64, 128), F32),
        V((32, 128), F32), V((4, 8, 128), BF16), V((32, 8, 128), BF16), V((256, 128), F32),
        V((32, 8, 128), F32), V((32, 128), F32),
        V((32, 128), BF16), V((64, 32, 128), BF16), V((2048, 128), F32), V((SLOTS, D), BF16), V((SLOTS, D), BF16),
        V((SLOTS, D), BF16),
        V((2, SLOTS, 1024), BF16), V((SLOTS, 1024), BF16), V((128, 16, 128), BF16), V((128, 16, 128), BF16),
        V((32, 128), F32),
        V((256, 128), F32), V((2 * SLOTS, 128), BF16), V((256, 128), F32),
        pltpu.SemaphoreType.DMA((10,)), pltpu.SemaphoreType.DMA((24,)), pltpu.SemaphoreType.DMA((24,)),
        pltpu.SemaphoreType.REGULAR,
    ]
    shapes = (
        jax.ShapeDtypeStruct((2, D), BF16),
        jax.ShapeDtypeStruct((2, 512), BF16),
        jax.ShapeDtypeStruct((2, 512), BF16),
    )
    results = pl.pallas_call(
        kernel,
        out_shape=shapes,
        in_specs=[smem, smem] + [vmem] * 7 + [hbm] * 12,
        out_specs=(vmem, vmem, vmem),
        scratch_shapes=scratch,
        compiler_params=pltpu.CompilerParams(
            collective_id=0, has_side_effects=True, vmem_limit_bytes=56 * 1024 * 1024
        ),
    )(
        lengths, lam_heads, hidden_in, inv,
        attn_gain.reshape(16, 128), moe_gain.reshape(16, 128), head_gain.reshape(1, 256),
        routing.T, route_weight.T,
        key_cache, value_cache, query_w, key_w, value_w, out_w, gate_w, up_w, down_w,
        shared_gate, shared_up, shared_down,
    )
    return pl.pallas_call(
        hand_over, out_shape=shapes, in_specs=[vmem] * 3, out_specs=(vmem,) * 3
    )(*results)


def solution(mesh):
    row, cube, whole = P("ep", None), P("ep", None, None), P()
    return jax.shard_map(
        on_device,
        mesh=mesh,
        in_specs=(
            row, P("ep"), cube, cube, row, row, row, row, whole, whole,
            whole, whole, whole, whole, cube, cube, cube, whole, whole, whole,
        ),
        out_specs=(row, row, row),
        check_vma=False,
    )
```

```python
import functools

import jax
import jax.numpy as jnp
import numpy as np
from jax import lax
from jax.experimental import pallas as pl
from jax.experimental.pallas import tpu as pltpu
from jax.sharding import PartitionSpec as P

MESH = pl.DeviceIdType.MESH
F32 = jnp.float32
BF16 = jnp.bfloat16
SIDE = 4
CHIPS = SIDE**3
PLANE = SIDE * SIDE * 2
ISSUE = (2, 1, 3, 0)
ARRIVE = (1, 3, 0, 2)
SLOTS = 32
D = 2048
eps_norm = 1e-06
eps_head = 1e-05
theta_base = 500000.0


def bytes_of(buf, count, sem):
    part = buf.at[pl.ds(0, count)]
    pltpu.make_async_copy(part, part, sem).wait()


def row_parity():
    return lax.broadcasted_iota(jnp.int32, (32, 128), 0) % 2


def fold_rms(fold, gain):
    parity = row_parity()
    squares = fold * fold
    first = jnp.sum(jnp.where(parity == 0, squares, 0.0), keepdims=True)
    second = jnp.sum(jnp.where(parity == 1, squares, 0.0), keepdims=True)
    r0 = lax.rsqrt(first * (1.0 / D) + eps_norm)
    r1 = lax.rsqrt(second * (1.0 / D) + eps_norm)
    return fold * jnp.where(parity == 0, r0, r1) * gain


def kernel(
    len_ref, lam_ref, hidden_ref, inv_ref, again_ref, mgain_ref, hgain_ref, routing_ref, rweight_ref,
    kc_hbm, vc_hbm, qw_hbm, kw_hbm, vw_hbm, ow_hbm, gate_hbm, up_hbm, down_hbm, sg_hbm, su_hbm, sd_hbm,
    layer_ref, kout_ref, vout_ref,
    kc, vc, gate, up, down, sg, su, sd,
    wcat, owcat, wrecv, owrecv,
    hid, gdup, asend, acts, xf, p2, qkv_in, qs,
    af, asend2, acts2, p5, oin, proj,
    ms, mrecv, big, pk, pgive, ptake, rs, rpar, esend, erecv, shf,
    pt, ptt, ptmp,
    local_sem, send_sem, recv_sem, ready_sem,
):
    me = lax.axis_index("ep")
    c = me % 2
    p = me // 2
    x = p % SIDE
    y = (p // SIDE) % SIDE
    z = p // (SIDE * SIDE)
    xc = x * 2 + c
    partner = me + 1 - 2 * c
    o_me = z * 8 + xc
    w_me = y * 8 + xc

    def local(src, dst, k):
        cp = pltpu.make_async_copy(src, dst, local_sem.at[k])
        cp.start()
        return cp

    def remote(src, dst, k, target):
        pltpu.make_async_remote_copy(
            src_ref=src,
            dst_ref=dst,
            send_sem=send_sem.at[k],
            recv_sem=recv_sem.at[k],
            device_id=(target,),
            device_id_type=MESH,
        ).start()

    def line_of(k):
        return ((z * SIDE + y) * SIDE + (x + k // 2) % SIDE) * 2 + (c + k % 2) % 2

    barrier = pltpu.get_barrier_semaphore()

    def greet(sem, target):
        pl.semaphore_signal(sem, inc=1, device_id=(target,), device_id_type=MESH)

    for k in range(1, 8):
        greet(barrier, line_of(k))
    for k in range(1, SIDE):
        greet(barrier, ((z * SIDE + (y + k) % SIDE) * SIDE + x) * 2 + c)
        greet(barrier, (((z + k) % SIDE * SIDE + y) * SIDE + x) * 2 + c)

    for h in range(8):
        local(qw_hbm.at[:, pl.ds(h * 256, 256)], wcat.at[h, :, pl.ds(0, 256)], 0)
        kv_hbm = kw_hbm if h < 4 else vw_hbm
        local(kv_hbm.at[:, pl.ds((h % 4) * 128, 128)], wcat.at[h, :, pl.ds(256, 128)], 0)

    wide = hidden_ref[...].astype(F32)
    for s in range(16):
        hid[2 * s : 2 * s + 2, :] = wide[:, 128 * s : 128 * s + 128]
    hidden = hid[...]

    def doubled(gain_ref):
        gdup[pl.ds(0, 16, stride=2), :] = gain_ref[...]
        gdup[pl.ds(1, 16, stride=2), :] = gain_ref[...]
        return gdup[...]

    asend[...] = fold_rms(hidden, doubled(again_ref)).astype(BF16).reshape(4, 8, 128)
    pltpu.make_async_copy(wcat, wcat, local_sem.at[0]).wait()
    for h in range(8):
        local(ow_hbm.at[:, pl.ds(h * 256, 256)], owcat.at[h], 1)
    c_kc = local(kc_hbm, kc, 2)
    c_vc = local(vc_hbm, vc, 3)
    c_sg = local(sg_hbm, sg, 4)
    c_su = local(su_hbm, su, 5)
    c_sd = local(sd_hbm, sd, 6)
    c_gate = local(gate_hbm.at[0], gate, 7)
    c_up = local(up_hbm.at[0], up, 8)
    c_down = local(down_hbm.at[0], down, 9)

    pl.semaphore_wait(barrier, 13)
    for k in range(1, 8):
        greet(ready_sem, line_of(k))
    pl.semaphore_wait(ready_sem, 7)

    def owner_of(k):
        dz, dx, dc = k // 8, (k // 2) % 4, k % 2
        zt, xt, ct = (z + dz) % SIDE, (x + dx) % SIDE, (c + dc) % 2
        return zt, xt * 2 + ct, ((zt * SIDE + y) * SIDE + xt) * 2 + ct

    def holder_of(k):
        dy, dx, dc = k // 8, (k // 2) % 4, k % 2
        yt, xt, ct = (y + dy) % SIDE, (x + dx) % SIDE, (c + dc) % 2
        return xt * 2 + ct, ((z * SIDE + yt) * SIDE + xt) * 2 + ct

    def send_acts(k, _):
        zt, _, target = owner_of(k)
        remote(asend.at[zt], acts.at[o_me], 0, target)
        return 0

    def send_w(k, _):
        ht, target = holder_of(k)
        remote(wcat.at[ht], wrecv.at[w_me], 1, target)
        return 0

    lax.fori_loop(1, PLANE, send_acts, 0)
    lax.fori_loop(1, PLANE, send_w, 0)
    acts[o_me] = asend[z]
    wrecv[w_me] = wcat[xc]

    upto = (
        lax.broadcasted_iota(jnp.int32, (256, 256), 0)
        <= lax.broadcasted_iota(jnp.int32, (256, 256), 1)
    ).astype(BF16)
    slot = lax.broadcasted_iota(jnp.int32, (SLOTS, 256), 0).astype(F32)
    tables = []
    for expert in (me, partner):
        match = routing_ref[...] == expert
        here = jnp.max(jnp.where(match, 1.0, 0.0), axis=0, keepdims=True)
        rows = jnp.broadcast_to(here, (8, 256)).astype(BF16)
        place = jnp.dot(rows, upto, preferred_element_type=F32)[0:1] - 1.0
        tables.append(jnp.where((place == slot) & (here > 0.0), 1.0, 0.0))
        if expert is me:
            weight = jnp.sum(jnp.where(match, rweight_ref[...], 0.0), axis=0, keepdims=True)
            slot_w = jnp.sum(tables[0] * weight, axis=1, keepdims=True)
    tables.append(jnp.zeros((128 - 2 * SLOTS, 256), F32))
    ptmp[...] = jnp.transpose(jnp.concatenate(tables, axis=0))
    for zq in range(SIDE):
        for ct in range(4):
            at = zq * 64 + ct * 16
            pt[at : at + 16, :] = ptmp[pl.ds(zq * 64 + ct, 16, stride=4), :]
    seen = jnp.concatenate(
        [ptmp[pl.ds(c * 2 + t, 64, stride=4), :] for t in range(2)], axis=0
    )
    ptt[...] = jnp.transpose(seen)[0 : 2 * SLOTS].astype(BF16)

    half_sign = jnp.where(lax.broadcasted_iota(jnp.int32, (1, 128), 1) < 64, -1.0, 1.0)
    turns = []
    for t in range(2):
        angle = len_ref[t].astype(F32) * inv_ref[...]
        turns.append((jnp.cos(angle), jnp.sin(angle) * half_sign))

    def columns_of(arrived):
        xf[...] = arrived[...].astype(F32).reshape(256, 128)
        rows = [
            jnp.concatenate(
                [xf[pl.ds(2 * s + t, 32, stride=8), :] for t in range(2)], axis=0
            )
            for s in range(4)
        ]
        return jnp.concatenate(rows, axis=1).astype(BF16)

    bytes_of(acts, PLANE - 1, recv_sem.at[0])
    bytes_of(wrecv, PLANE - 1, recv_sem.at[1])
    part = jnp.dot(
        columns_of(acts), wrecv[...].reshape(512, 384), preferred_element_type=F32
    )
    for b in range(3):
        for t in range(2):
            p2[pl.ds(2 * b + t, 32, stride=8), :] = part[
                32 * t : 32 * t + 32, 128 * b : 128 * b + 128
            ]
    for t in range(2):
        p2[pl.ds(6 + t, 32, stride=8), :] = jnp.zeros((32, 128), F32)

    def send_part(k, _):
        zt, ht, target = owner_of(k)
        ot = pl.multiple_of((zt * 8 + ht) * 8, 8)
        remote(p2.at[pl.ds(ot, 8), :], qkv_in.at[o_me], 2, target)
        return 0

    lax.fori_loop(1, PLANE, send_part, 0)
    qkv_in[o_me] = p2[pl.ds(pl.multiple_of(o_me * 8, 8), 8), :]

    pltpu.make_async_copy(owcat, owcat, local_sem.at[1]).wait()

    def send_ow(k, _):
        ht, target = holder_of(k)
        remote(owcat.at[ht], owrecv.at[w_me], 3, target)
        return 0

    lax.fori_loop(1, PLANE, send_ow, 0)
    owrecv[w_me] = owcat[xc]
    c_kc.wait()
    c_vc.wait()

    bytes_of(qkv_in, PLANE - 1, recv_sem.at[2])
    total = qkv_in[0:8]
    for k in range(1, 4):
        total = total + qkv_in[8 * k : 8 * k + 8]
    qs[...] = total.reshape(64, 128)

    scale = 128.0**-0.5
    row16 = lax.broadcasted_iota(jnp.int32, (16, 128), 0)
    row8 = lax.broadcasted_iota(jnp.int32, (8, 1), 0)
    lam = jnp.zeros((8, 1), F32)
    for h in range(8):
        lam = jnp.where(row8 == h, lam_ref[h], lam)
    keys, values = [], []
    for t in range(2):
        cos, sin = turns[t]

        def turn(v):
            return v * cos + pltpu.roll(v, 64, 1) * sin

        kv = qs[pl.ds(4 + t, 8, stride=8), :]
        q16 = jnp.concatenate(
            [turn(qs[pl.ds(t, 8, stride=8), :]), turn(qs[pl.ds(2 + t, 8, stride=8), :])],
            axis=0,
        )
        q16 = q16.astype(BF16).astype(F32)
        kn = turn(kv).astype(BF16).astype(F32)
        vn = kv.astype(BF16).astype(F32)
        keys.append(jnp.concatenate([kn[i : i + 1] for i in range(4)], axis=1))
        vflat = jnp.concatenate([vn[i : i + 1] for i in range(4, 8)], axis=1)
        values.append(vflat)
        own_keys = jnp.concatenate(
            [jnp.broadcast_to(kn[i : i + 1], (4, 128)) for i in (0, 2, 1, 3)], axis=0
        )
        self_score = jnp.sum(q16 * own_keys, axis=1, keepdims=True) * scale
        blocks = []
        for k in range(2):
            for j in range(2):
                lo = j * 8 + k * 4
                blocks.append(jnp.where((row16 >= lo) & (row16 < lo + 4), q16, 0.0))
        wide_q = jnp.concatenate(blocks, axis=1).astype(BF16)
        scores = (
            lax.dot_general(
                wide_q, kc[t], (((1,), (1,)), ((), ())), preferred_element_type=F32
            )
            * scale
        )
        live = lax.broadcasted_iota(jnp.int32, (16, 1024), 1) < len_ref[t]
        peak = jnp.maximum(
            jnp.max(jnp.where(live, scores, -jnp.inf), axis=1, keepdims=True), self_score
        )
        weights = jnp.where(live, jnp.exp(scores - peak), 0.0)
        self_w = jnp.exp(self_score - peak)
        totals = jnp.sum(weights, axis=1, keepdims=True) + self_w
        comb = weights[0:8] / totals[0:8] - lam * weights[8:16] / totals[8:16]
        self_comb = self_w[0:8] / totals[0:8] - lam * self_w[8:16] / totals[8:16]
        out = jnp.dot(comb.astype(BF16), vc[t], preferred_element_type=F32)
        out = out + self_comb.astype(BF16).astype(F32) * vflat
        head = jnp.where(row8 < 4, out[:, 0:256], out[:, 256:512])
        mean = jnp.sum(head * head, axis=1, keepdims=True) * (1.0 / 256)
        head = head * lax.rsqrt(mean + eps_head) * hgain_ref[...]
        for half in range(2):
            af[pl.ds(2 * half + t, 8, stride=4), :] = head[:, 128 * half : 128 * half + 128]
    kout_ref[...] = jnp.concatenate(keys, axis=0).astype(BF16)
    vout_ref[...] = jnp.concatenate(values, axis=0).astype(BF16)
    asend2[...] = af[...].astype(BF16).reshape(4, 8, 128)

    def send_acts2(k, _):
        zt, _, target = owner_of(k)
        remote(asend2.at[zt], acts2.at[o_me], 4, target)
        return 0

    lax.fori_loop(1, PLANE, send_acts2, 0)
    acts2[o_me] = asend2[z]
    mgain = doubled(mgain_ref)
    bytes_of(owrecv, PLANE - 1, recv_sem.at[3])
    bytes_of(acts2, PLANE - 1, recv_sem.at[4])
    part = jnp.dot(
        columns_of(acts2), owrecv[...].reshape(512, 256), preferred_element_type=F32
    )
    for b in range(2):
        for t in range(2):
            p5[:, 2 * b + t, :] = part[32 * t : 32 * t + 32, 128 * b : 128 * b + 128]

    def send_part2(k, _):
        zt, ht, target = owner_of(k)
        remote(p5.at[zt * 8 + ht], oin.at[o_me], 5, target)
        return 0

    lax.fori_loop(1, PLANE, send_part2, 0)
    oin[o_me] = p5[o_me]
    bytes_of(oin, PLANE - 1, recv_sem.at[5])
    total = oin[0:8]
    for k in range(1, 4):
        total = total + oin[8 * k : 8 * k + 8]
    for h in range(8):
        proj[4 * h : 4 * h + 4, :] = total[h]
    mixed = (hidden + proj[...].astype(BF16).astype(F32)).astype(BF16).astype(F32)
    moe = fold_rms(mixed, mgain).astype(BF16)
    ms[...] = moe

    def chip_at(dz, k):
        zt, yt, xt = (z + dz) % SIDE, (y + k // SIDE) % SIDE, (x + k % SIDE) % SIDE
        return (zt * SIDE + yt) * SIDE + xt

    def group(dz):
        return pl.multiple_of((z - dz + SIDE) % SIDE * 16, 16), 16 if dz else 15

    for dz in ISSUE:

        def send_moe(k, _, dz=dz):
            remote(ms, mrecv.at[p], 12 + dz, chip_at(dz, k) * 2 + c)
            return 0

        lax.fori_loop(0 if dz else 1, 16, send_moe, 0)
    mrecv[p] = moe

    moe32 = moe.astype(F32)
    lhs = jnp.concatenate([moe32[2 * s : 2 * s + 2] for s in range(16)], axis=1).astype(BF16)
    c_sg.wait()
    c_su.wait()
    c_sd.wait()
    g = jnp.dot(lhs, sg[...], preferred_element_type=F32)
    u = jnp.dot(lhs, su[...], preferred_element_type=F32)
    shared = jnp.dot(
        (jax.nn.silu(g) * u).astype(BF16), sd[...], preferred_element_type=F32
    )
    for s in range(16):
        shf[2 * s : 2 * s + 2, :] = shared[:, 128 * s : 128 * s + 128]
    c_gate.wait()
    c_up.wait()
    c_down.wait()

    for dz in ARRIVE:
        first, count = group(dz)
        bytes_of(mrecv, count, recv_sem.at[12 + dz])
        for i in range(4):
            start = pl.multiple_of((first + 4 * i) * 32, 128)
            big[pl.ds(start, 128), :] = (
                mrecv[pl.ds(first + 4 * i, 4)].astype(F32).reshape(128, 128)
            )
    for s in range(8):
        rows = jnp.concatenate(
            [
                jnp.concatenate(
                    [big[pl.ds(4 * s + 2 * i + t, 64, stride=32), :] for t in range(2)], axis=0
                )
                for i in range(2)
            ],
            axis=1,
        ).astype(BF16)
        picked = jnp.dot(ptt[...], rows, preferred_element_type=F32).astype(BF16)
        pk[:, 256 * s : 256 * s + 256] = picked[0:SLOTS]
        pgive[:, 256 * s : 256 * s + 256] = picked[SLOTS : 2 * SLOTS]
    remote(pgive, ptake, 7, partner)
    bytes_of(ptake, SLOTS, recv_sem.at[7])
    pk[...] = (pk[...].astype(F32) + ptake[...].astype(F32)).astype(BF16)
    g = jnp.dot(pk[...], gate[...], preferred_element_type=F32)
    u = jnp.dot(pk[...], up[...], preferred_element_type=F32)
    hidden_e = (jax.nn.silu(g) * u).astype(BF16)
    for i in range(2):
        made = jnp.dot(
            hidden_e, down[:, 1024 * i : 1024 * i + 1024], preferred_element_type=F32
        ).astype(BF16)
        rs[i] = (made.astype(F32) * slot_w).astype(BF16)

    remote(rs.at[1 - c], rpar, 8, partner)
    bytes_of(rpar, SLOTS, recv_sem.at[8])
    pair = jnp.concatenate([rs[c], rpar[...]], axis=0)
    for dz in ISSUE:
        zt = (z + dz) % SIDE
        rows = pt[pl.ds(pl.multiple_of(zt * 64, 64), 64), 0 : 2 * SLOTS].astype(BF16)
        both = jnp.dot(rows, pair, preferred_element_type=F32)
        for ct in range(4):
            for s in range(8):
                big[pl.ds(dz * 512 + (ct // 2) * 16 + 2 * s + ct % 2, 16, stride=32), :] = both[
                    16 * ct : 16 * ct + 16, 128 * s : 128 * s + 128
                ]
        for i in range(4):
            at = dz * 512 + i * 128
            esend[pl.ds((zt * 16 + 4 * i) * 2, 8)] = (
                big[at : at + 128, :].astype(BF16).reshape(8, 16, 128)
            )

        def send_back(k, _, dz=dz):
            chip, core = chip_at(dz, k // 2), (c + k % 2) % 2
            device = chip * 2 + core
            remote(esend.at[device], erecv.at[c * CHIPS + p], 20 + dz, device)
            return 0

        lax.fori_loop(0 if dz else 1, 32, send_back, 0)
    erecv[c * CHIPS + p] = esend[me]
    halves = [jnp.zeros((16, 128), F32)] * 2
    for dz in ARRIVE:
        first, count = group(dz)
        bytes_of(erecv, 16 + count, recv_sem.at[20 + dz])
        for half in range(2):
            for i in range(2):
                rows = erecv[pl.ds(half * CHIPS + first + 8 * i, 8)].astype(F32)
                halves[half] = halves[half] + jnp.sum(rows, axis=0)
    routed = jnp.concatenate(halves, axis=0)
    layer = mixed + routed + shf[...]
    layer_ref[...] = jnp.concatenate(
        [layer[2 * s : 2 * s + 2] for s in range(16)], axis=1
    ).astype(BF16)

    bytes_of(acts, PLANE - 1, send_sem.at[0])
    bytes_of(wrecv, PLANE - 1, send_sem.at[1])
    bytes_of(qkv_in, PLANE - 1, send_sem.at[2])
    bytes_of(owrecv, PLANE - 1, send_sem.at[3])
    bytes_of(acts2, PLANE - 1, send_sem.at[4])
    bytes_of(oin, PLANE - 1, send_sem.at[5])
    bytes_of(ptake, SLOTS, send_sem.at[7])
    bytes_of(rpar, SLOTS, send_sem.at[8])
    for dz in range(SIDE):
        count = 16 if dz else 15
        bytes_of(mrecv, count, send_sem.at[12 + dz])
        bytes_of(erecv, 16 + count, send_sem.at[20 + dz])


def hand_over(*refs):
    for i in range(3):
        refs[3 + i][...] = refs[i][...]


def on_device(
    hidden_in, lengths, key_cache, value_cache, query_w, key_w, value_w, out_w, lam_heads, head_gain,
    attn_gain, moe_gain, routing, route_weight, gate_w, up_w, down_w, shared_gate, shared_up, shared_down,
):
    inv = (theta_base ** (-np.arange(64, dtype=np.float32) / 64)).astype(np.float32)
    inv = jnp.asarray(np.tile(inv, 2)[None])
    vmem = pl.BlockSpec(memory_space=pltpu.VMEM)
    smem = pl.BlockSpec(memory_space=pltpu.SMEM)
    hbm = pl.BlockSpec(memory_space=pl.ANY)
    V = pltpu.VMEM
    scratch = [
        V((2, 1024, 512), BF16), V((2, 1024, 512), BF16),
        V((D, 512), BF16), V((D, 512), BF16), V((512, D), BF16),
        V((D, 512), BF16), V((D, 512), BF16), V((512, D), BF16),
        V((8, 16, 384), BF16), V((8, 16, 256), BF16), V((32, 16, 384), BF16), V((32, 16, 256), BF16),
        V((32, 128), F32), V((32, 128), F32), V((4, 8, 128), BF16), V((32, 8, 128), BF16),
        V((256, 128), F32), V((256, 128), F32), V((32, 8, 128), F32), V((64, 128), F32),
        V((32, 128), F32), V((4, 8, 128), BF16), V((32, 8, 128), BF16), V((32, 4, 128), F32),
        V((32, 4, 128), F32), V((32, 128), F32),
        V((32, 128), BF16), V((64, 32, 128), BF16), V((2048, 128), F32), V((SLOTS, D), BF16), V((SLOTS, D), BF16),
        V((SLOTS, D), BF16),
        V((2, SLOTS, 1024), BF16), V((SLOTS, 1024), BF16), V((128, 16, 128), BF16), V((128, 16, 128), BF16),
        V((32, 128), F32),
        V((256, 128), F32), V((2 * SLOTS, 128), BF16), V((256, 128), F32),
        pltpu.SemaphoreType.DMA((10,)), pltpu.SemaphoreType.DMA((24,)), pltpu.SemaphoreType.DMA((24,)),
        pltpu.SemaphoreType.REGULAR,
    ]
    shapes = (
        jax.ShapeDtypeStruct((2, D), BF16),
        jax.ShapeDtypeStruct((2, 512), BF16),
        jax.ShapeDtypeStruct((2, 512), BF16),
    )
    results = pl.pallas_call(
        kernel,
        out_shape=shapes,
        in_specs=[smem, smem] + [vmem] * 7 + [hbm] * 12,
        out_specs=(vmem, vmem, vmem),
        scratch_shapes=scratch,
        compiler_params=pltpu.CompilerParams(
            collective_id=0, has_side_effects=True, vmem_limit_bytes=56 * 1024 * 1024
        ),
    )(
        lengths, lam_heads, hidden_in, inv,
        attn_gain.reshape(16, 128), moe_gain.reshape(16, 128), head_gain.reshape(1, 256),
        routing.T, route_weight.T,
        key_cache, value_cache, query_w, key_w, value_w, out_w, gate_w, up_w, down_w,
        shared_gate, shared_up, shared_down,
    )
    return pl.pallas_call(
        hand_over, out_shape=shapes, in_specs=[vmem] * 3, out_specs=(vmem,) * 3
    )(*results)


def solution(mesh):
    row, cube, whole = P("ep", None), P("ep", None, None), P()
    return jax.shard_map(
        on_device,
        mesh=mesh,
        in_specs=(
            row, P("ep"), cube, cube, row, row, row, row, whole, whole,
            whole, whole, whole, whole, cube, cube, cube, whole, whole, whole,
        ),
        out_specs=(row, row, row),
        check_vma=False,
    )
```
